32 devices in a mesh: ep: 16 (over z, y, x), tp: 2 (over core).
Axes of the slice: x: 2, y: 2, z: 4, core: 2. Of those that a mesh axis runs over, the one named last changes fastest.
Arguments:
- residual: bfloat16 [1024, 2048], P('ep', 'tp'), may hold values from -100 to 100
- route_ids: int32 [1024, 4], P('ep'), may hold values from 0 to 15, all different within a row; in each aligned block of 64 rows (0 to 63, 64 to 127, ...) at most 24 rows name the same one
- route_weights: float32 [1024, 4], P('ep'), may hold values from 0.1 to 1
- carried_state: float32 [2, 1024, 4096], P(None, 'ep', 'tp'), may hold values from -6 to 6
- mix_gain: float32 [2048], replicated, may hold values from 0.1 to 1.9
- in_proj: bfloat16 [2048, 1024], P(None, 'tp'), may hold values from -0.125 to 0.125
- decay_rate: float32 [64, 64], P('tp'), may hold values from 0.1 to 2
- frequency: float32 [64, 64], P('tp'), may hold values from -3 to 3
- step_size: float32 [64], P('tp'), may hold values from 0.05 to 1
- input_map: float32 [2, 64, 64, 16], P(None, 'tp'), may hold values from -1.5 to 1.5
- output_matrix: float32 [2, 64, 16, 64], P(None, 'tp'), may hold values from -0.5 to 0.5
- passthrough_scale: float32 [1024], P('tp'), may hold values from -4 to 4
- out_gain: float32 [1024], replicated, may hold values from 0.1 to 1.9
- out_proj: bfloat16 [1024, 2048], P(None, 'tp'), may hold values from -0.1875 to 0.1875
- ffn_gain: float32 [2048], replicated, may hold values from 0.1 to 1.9
- w_gate: bfloat16 [16, 2048, 2048], P('ep', None, 'tp'), may hold values from -5 to 5
- w_up: bfloat16 [16, 2048, 2048], P('ep', None, 'tp'), may hold values from -5 to 5
- w_down: bfloat16 [16, 2048, 2048], P('ep', 'tp'), may hold values from -0.125 to 0.125
Outputs:
- updated: bfloat16 [1024, 2048], P('ep', 'tp')
- new_state: float32 [2, 1024, 4096], P(None, 'ep', 'tp')
The draws below stay inside these ranges and needn't reach their ends.
Inputs may be any that keep to these rules, and one draw needn't show every extreme that they name: `route_ids`: each row names 4 different experts. Among the 64 rows of one device (aligned blocks) no expert is named more than 24 times, and in every draw some block names some expert exactly 24 times.
All inputs are finite; a program needn't handle non-finite values.
Results may differ from the reference program's by a relative error of at most 0.018.
Values may be sent and summed in bfloat16 or wider, within the bound.
A program may use at most 128 MiB of HBM per device.

```python
import math
import jax
import jax.numpy as jnp
import numpy as np
from jax import lax

D = 2048
S5W = 1024
GROUP_CH = 16
GROUPS = 64
STATE = 64
FF = 2048
EXPERTS = 16
TOPK = 4
SEQ_DEV = 64
TOKENS = 1024
CAP = 24
WIDTH_SPLIT = 2
N_EP = 16


def draw_residual(key, part):
    key_one = jax.random.fold_in(key, 11)
    key_three = jax.random.fold_in(key, 13)
    column_pos = jnp.arange(D, dtype=jnp.float32) / D
    column_ramp = jnp.exp(math.log(3.0) * column_pos)
    base_draw = jnp.clip(jax.random.normal(key_one, (TOKENS, D), jnp.float32), -5.0, 5.0)
    jitter = jnp.exp(jax.random.uniform(key_three, (1, D), jnp.float32, -0.35, 0.35))
    return (base_draw * column_ramp * jitter / 1.5).astype(jnp.bfloat16)


def expert_weight(key, salt_value):
    key_one = jax.random.fold_in(key, salt_value)
    key_two = jax.random.fold_in(key, salt_value + 1)
    base_draw = jnp.clip(jax.random.normal(key_one, (EXPERTS, D, FF), jnp.float32), -5.0, 5.0) / math.sqrt(D)
    top_scale = 3.0
    column_scale = 0.5 * jnp.exp(jax.random.uniform(key_two, (EXPERTS, 1, FF), jnp.float32, 0.0, math.log(top_scale / 0.5)))
    return (base_draw * column_scale).astype(jnp.bfloat16)


def draw_w_gate(key, part):
    return expert_weight(key, 21)


def draw_w_up(key, part):
    return expert_weight(key, 31)


def block_levels(stream_key, dims, split, smallest, largest):
    factor_of = 1.0
    for axis_at, shards_of in split:
        heights = jax.random.uniform(jax.random.fold_in(jax.random.fold_in(stream_key, 6), axis_at), (shards_of,), jnp.float32, smallest / len(split), largest / len(split))
        factor_of = factor_of * jnp.repeat(jnp.exp(heights), dims[axis_at] // shards_of).reshape((-1,) + (1,) * (len(dims) - 1 - axis_at))
    return factor_of


def deal_out(own_key, own, number, rows, count, top, limit, lean):
    ranking = jax.random.permutation(own_key, count)
    packed, common = load_shares(count, rows * top, limit, lean, True), load_shares(count, rows * top, limit, lean, False)
    places = jnp.arange(count)

    def named(tallies, turn):
        used = int((tallies > 0).sum())
        fixed = max(1, used // 4)
        moved = fixed + (places - fixed + turn * (used - fixed)) % max(1, count - fixed)
        return jnp.zeros((count,), jnp.int32).at[ranking[jnp.where(places < fixed, places, moved)]].set(jnp.asarray(tallies, jnp.int32))

    tallies = jnp.where(number % 4 == 0, named(packed, number // 4), named(common, number - number // 4 - 1))
    mixed = jax.random.permutation(jax.random.fold_in(own, 3), count)
    source_of, taker = mixed[0:count // 2 * 2:2], mixed[1:count // 2 * 2:2]
    slack = jnp.minimum(tallies[source_of] - 1, limit - tallies[taker]) // 2
    slack = jnp.where((source_of == ranking[0]) | (taker == ranking[0]) | (tallies[taker] == 0), 0, jnp.maximum(slack, 0))
    moved = jax.random.randint(jax.random.fold_in(own, 4), (count // 2,), 0, 1 << 20) % (slack + 1)
    tallies = tallies.at[source_of].add(-moved).at[taker].add(moved)
    labels = jnp.searchsorted(jnp.cumsum(tallies), jnp.arange(rows * top), side="right").astype(jnp.int32)
    grid = labels.reshape(top, rows).T
    grid = grid[jax.random.permutation(jax.random.fold_in(own, 1), rows)]
    turn = jax.random.randint(jax.random.fold_in(own, 2), (rows, 1), 0, top)
    return jnp.take_along_axis(grid, (jnp.arange(top)[None, :] + turn) % top, axis=1)


def load_shares(count, total, bound, slope, full):
    portions = [(1 << 20) // math.isqrt(grade ** slope) + 1 for grade in range(1, count + 1)]
    largest = bound if full else min(bound, max(-(-total // count), total * portions[0] // sum(portions)))
    least = 1 if total - largest >= count - 1 else 0
    counts, surplus = [largest] + [least] * (count - 1), total - largest - least * (count - 1)
    while surplus > 0:
        free = [i for i in range(1, count) if counts[i] < largest] or [i for i in range(1, count) if counts[i] < bound]
        pool, left = sum([portions[i] for i in free]), surplus
        for i in free:
            addition = min(bound - counts[i], max(1, left * portions[i] // pool), surplus)
            counts[i] = counts[i] + addition
            surplus = surplus - addition
    return np.array(counts)


def scatter_about(own_key, shape, scale, bound, cuts=(), kind=jnp.bfloat16):
    factor_of = block_levels(own_key, shape, cuts, -0.22, 0.18) if cuts else 1.0
    entries = jax.random.normal(own_key, shape, jnp.float32) * scale * factor_of
    return jnp.minimum(jnp.maximum(entries, -bound), bound).astype(kind)


def setup_inputs(seed: int = 0) -> dict:
    arg_keys = jax.random.split(jax.random.key(seed), 19)
    residual = draw_residual(jax.random.fold_in(arg_keys[18], 71), 0)
    route_ids_keys = jax.random.split(jax.random.fold_in(arg_keys[1], 1), TOKENS // SEQ_DEV)
    route_ids_turns = jax.random.permutation(jax.random.fold_in(arg_keys[1], 3), TOKENS // SEQ_DEV)
    route_ids = jax.vmap(lambda own, number: deal_out(jax.random.fold_in(arg_keys[1], 2), own, number, SEQ_DEV, EXPERTS, TOPK, CAP, 1))(route_ids_keys, route_ids_turns).reshape((TOKENS, TOPK))
    route_weights = jnp.clip(0.1 + 0.9 * jax.random.uniform(arg_keys[2], (TOKENS, TOPK), jnp.float32) ** block_levels(arg_keys[2], (TOKENS, TOPK), ((0, 16),), -0.2, 0.2), 0.1, 1.0)
    carried_state = scatter_about(arg_keys[3], (2, TOKENS, GROUPS * STATE), 1.0, 6.0, ((1, 16), (2, 2)), jnp.float32)
    mix_gain = jnp.clip(1.0 + 0.18 * jax.random.normal(arg_keys[4], (D,), jnp.float32), 0.1, 1.9)
    in_proj = scatter_about(arg_keys[5], (D, S5W), D ** -0.5, 0.125, ((1, 2),))
    decay_rate = jnp.clip(jnp.exp(math.log(2.0) - 2.9957323 * jax.random.uniform(arg_keys[6], (GROUPS, STATE), jnp.float32) ** block_levels(arg_keys[6], (GROUPS, STATE), ((0, 2),), -0.2, 0.2)), 0.1, 2.0)
    frequency = jnp.clip(jax.random.uniform(arg_keys[7], (GROUPS, STATE), jnp.float32, -3.0, 3.0) * block_levels(arg_keys[7], (GROUPS, STATE), ((0, 2),), -0.4, 0.0), -3.0, 3.0)
    step_size = jnp.clip(jnp.exp(math.log(1.0) - 2.9957323 * jax.random.uniform(arg_keys[8], (GROUPS,), jnp.float32) ** block_levels(arg_keys[8], (GROUPS,), ((0, 2),), -0.2, 0.2)), 0.05, 1.0)
    input_map = scatter_about(arg_keys[9], (2, GROUPS, STATE, GROUP_CH), GROUP_CH ** -0.5, 1.5, ((1, 2),), jnp.float32)
    output_matrix = scatter_about(arg_keys[10], (2, GROUPS, GROUP_CH, STATE), (2 * STATE) ** -0.5, 0.5, ((1, 2),), jnp.float32)
    passthrough_scale = scatter_about(arg_keys[11], (S5W,), 1.0, 4.0, ((0, 2),), jnp.float32)
    out_gain = jnp.clip(1.0 + 0.18 * jax.random.normal(arg_keys[12], (S5W,), jnp.float32), 0.1, 1.9)
    out_proj = scatter_about(arg_keys[13], (S5W, D), S5W ** -0.5, 0.1875, ((1, 2),))
    ffn_gain = jnp.clip(1.0 + 0.18 * jax.random.normal(arg_keys[14], (D,), jnp.float32), 0.1, 1.9)
    w_gate = draw_w_gate(jax.random.fold_in(arg_keys[18], 71), 0)
    w_up = draw_w_up(jax.random.fold_in(arg_keys[18], 71), 0)
    w_down = scatter_about(arg_keys[17], (EXPERTS, FF, D), FF ** -0.5, 0.125, ((0, 16), (1, 2)))
    return {"residual": residual, "route_ids": route_ids, "route_weights": route_weights, "carried_state": carried_state, "mix_gain": mix_gain, "in_proj": in_proj, "decay_rate": decay_rate, "frequency": frequency, "step_size": step_size, "input_map": input_map, "output_matrix": output_matrix, "passthrough_scale": passthrough_scale, "out_gain": out_gain, "out_proj": out_proj, "ffn_gain": ffn_gain, "w_gate": w_gate, "w_up": w_up, "w_down": w_down}


epsilon = 1e-06
clamp_limit = 7.0
swish_alpha = 1.702

def rms_rows(values, gain_vec):
    return values * lax.rsqrt(lax.optimization_barrier(jnp.mean(values * values, axis=1, keepdims=True)) + epsilon) * gain_vec

def discretize(decay_rate, frequency, step_size):
    rate_real = -decay_rate
    rate_imag = frequency
    time_step = step_size[:, None]
    magnitude = jnp.exp(rate_real * time_step)
    phase_angle = rate_imag * time_step
    bar_real = magnitude * jnp.cos(phase_angle)
    bar_imag = magnitude * jnp.sin(phase_angle)
    denominator = rate_real * rate_real + rate_imag * rate_imag
    shifted = bar_real - 1.0
    coef_real = (shifted * rate_real + bar_imag * rate_imag) / denominator
    coef_imag = (bar_imag * rate_real - shifted * rate_imag) / denominator
    return (bar_real, bar_imag, coef_real, coef_imag)

def state_step(channels, carried_state, decay_rate, frequency, step_size, input_map, output_matrix, passthrough_scale):
    row_count = channels.shape[0]
    number_of_groups, state_width = decay_rate.shape
    channels_per_group = input_map.shape[3]
    bar_real, bar_imag, coef_real, coef_imag = discretize(decay_rate, frequency, step_size)
    map_real = coef_real[..., None] * input_map[0] - coef_imag[..., None] * input_map[1]
    map_imag = coef_real[..., None] * input_map[1] + coef_imag[..., None] * input_map[0]
    input_rows = channels.astype(jnp.float32).reshape(row_count, number_of_groups, channels_per_group)
    largest_precision = lax.Precision.HIGHEST
    push_real = jnp.einsum('sgc,gpc->sgp', input_rows, map_real, precision=largest_precision)
    push_imag = jnp.einsum('sgc,gpc->sgp', input_rows, map_imag, precision=largest_precision)
    old_real = carried_state[0].reshape(row_count, number_of_groups, state_width)
    old_imag = carried_state[1].reshape(row_count, number_of_groups, state_width)
    updated_real = bar_real * old_real - bar_imag * old_imag + push_real
    updated_imaginary = bar_real * old_imag + bar_imag * old_real + push_imag
    mixer_output = jnp.einsum('dfk,idk->idf', output_matrix[0], updated_real, precision=largest_precision) - jnp.einsum('dfk,idk->idf', output_matrix[1], updated_imaginary, precision=largest_precision) + passthrough_scale.reshape(number_of_groups, channels_per_group) * input_rows
    activated = jax.nn.gelu(mixer_output.reshape(row_count, number_of_groups * channels_per_group)).astype(jnp.bfloat16)
    new_state = jnp.stack([updated_real.reshape(row_count, -1), updated_imaginary.reshape(row_count, -1)])
    return (activated, new_state)

def expert_apply(expert_item):
    rows_in, gate_w, up_w, down_w = expert_item
    slot_count = rows_in.shape[0]
    gate_pre = jnp.dot(rows_in, gate_w, preferred_element_type=jnp.float32)
    up_pre = jnp.dot(rows_in, up_w, preferred_element_type=jnp.float32)
    gated = jnp.minimum(gate_pre, clamp_limit)
    activation = ((jnp.clip(up_pre, -clamp_limit, clamp_limit) + 1.0) * gated * jax.nn.sigmoid(swish_alpha * gated)).astype(jnp.bfloat16)
    block_width = FF // WIDTH_SPLIT
    pieces = jnp.einsum('mtf,tfd->mtd', activation.reshape(slot_count, WIDTH_SPLIT, block_width).astype(jnp.float32), down_w.reshape(WIDTH_SPLIT, block_width, D).astype(jnp.float32))
    pieces = lax.optimization_barrier(pieces.astype(jnp.bfloat16)).astype(jnp.float32)
    return lax.optimization_barrier(jnp.sum(pieces, axis=1)).astype(jnp.bfloat16)

def reference(residual, route_ids, route_weights, carried_state, mix_gain, in_proj, decay_rate, frequency, step_size, input_map, output_matrix, passthrough_scale, out_gain, out_proj, ffn_gain, w_gate, w_up, w_down):
    start_rows = residual.astype(jnp.float32)
    normed_rows = rms_rows(start_rows, mix_gain).astype(jnp.bfloat16)
    channels = jnp.dot(normed_rows, in_proj, preferred_element_type=jnp.float32).astype(jnp.bfloat16)
    activated, new_state = state_step(channels, carried_state, decay_rate, frequency, step_size, input_map, output_matrix, passthrough_scale)
    scaled = rms_rows(activated.astype(jnp.float32), out_gain).astype(jnp.bfloat16)
    after_mixer = (start_rows + jnp.dot(scaled, out_proj, preferred_element_type=jnp.float32)).astype(jnp.bfloat16)
    expert_in = rms_rows(after_mixer.astype(jnp.float32), ffn_gain).astype(jnp.bfloat16)
    route_count = TOKENS * TOPK
    flat_ids = route_ids.reshape(route_count).astype(jnp.int32)
    onehot = (flat_ids[:, None] == jnp.arange(EXPERTS, dtype=jnp.int32)[None, :]).astype(jnp.int32)
    blocked = onehot.reshape(N_EP, SEQ_DEV * TOPK, EXPERTS)
    before = (jnp.cumsum(blocked, axis=1).astype(jnp.int32) - blocked).reshape(route_count, EXPERTS)
    slot_index = lax.optimization_barrier(jnp.sum(before * onehot, axis=1)).astype(jnp.int32)
    route_iota = jnp.arange(route_count, dtype=jnp.int32)
    block_index = (route_iota // (SEQ_DEV * TOPK)).astype(jnp.int32)
    slot_total = N_EP * CAP
    position = (flat_ids * slot_total + block_index * CAP + slot_index).astype(jnp.int32)
    source_row = (route_iota // TOPK).astype(jnp.int32)
    row_table = jnp.full((EXPERTS * slot_total,), TOKENS, dtype=jnp.int32).at[position].set(source_row)
    padded = jnp.concatenate([expert_in, jnp.zeros((1, D), jnp.bfloat16)], axis=0)
    gathered = padded[row_table].reshape(EXPERTS, slot_total, D)
    outputs = lax.map(expert_apply, (gathered, w_gate, w_up, w_down))
    picked = outputs.reshape(EXPERTS * slot_total, D)[position].reshape(TOKENS, TOPK, D)
    expert_sum = lax.optimization_barrier(jnp.sum(route_weights[:, :, None] * picked.astype(jnp.float32), axis=1))
    updated = (after_mixer.astype(jnp.float32) + expert_sum).astype(jnp.bfloat16)
    return (updated, new_state)
```

```python
import functools
import jax
import jax.numpy as jnp
from jax import lax
from jax.experimental import pallas as pl
from jax.experimental.pallas import tpu as pltpu
from jax.sharding import PartitionSpec as P

epsilon = 1e-06
clamp_limit = 7.0
swish_alpha = 1.702


def discretize(decay_rate, frequency, step_size):
    rate_real = -decay_rate
    time_step = step_size
    magnitude = jnp.exp(rate_real * time_step)
    phase_angle = frequency * time_step
    bar_real = magnitude * jnp.cos(phase_angle)
    bar_imag = magnitude * jnp.sin(phase_angle)
    denominator = rate_real * rate_real + frequency * frequency
    shifted = bar_real - 1.0
    coef_real = (shifted * rate_real + bar_imag * frequency) / denominator
    coef_imag = (bar_imag * rate_real - shifted * frequency) / denominator
    return (bar_real, bar_imag, coef_real, coef_imag)


def peer_of(index, offset):
    out = index
    bit = 1
    while bit <= offset:
        if offset & bit:
            out = out + bit * (1 - 2 * ((index // bit) % 2))
        bit *= 2
    return out


def gelu_tanh(value):
    inner = 0.7978845608028654 * (value + 0.044715 * value * value * value)
    return 0.5 * value * (1.0 + jnp.tanh(inner))


def row_squares(value):
    return jnp.sum(value * value, axis=1, keepdims=True)


def fill_transition(decay_ref, frequency_ref, step_ref, transition_ref):
    groups, entries = decay_ref.shape
    diagonal = lax.broadcasted_iota(jnp.int32, (groups, groups), 0) == lax.broadcasted_iota(
        jnp.int32, (groups, groups), 1
    )
    steps = jnp.sum(jnp.where(diagonal, step_ref[...], 0.0), axis=1, keepdims=True)
    shape = (groups, groups * entries)
    inside = (
        lax.broadcasted_iota(jnp.int32, shape, 0)
        == lax.broadcasted_iota(jnp.int32, shape, 1) // entries
    )
    for place, term in enumerate(discretize(decay_ref[...], frequency_ref[...], steps)):
        spread = jnp.concatenate([term] * groups, axis=1)
        transition_ref[place : place + 1, :] = jnp.sum(
            jnp.where(inside, spread, 0.0), axis=0, keepdims=True
        )


def fill_routes(capacity, ids_ref, route_weight_ref, taken_ref, combine_ref):
    top_count, rows = ids_ref.shape
    experts = taken_ref.shape[0] // capacity
    expert_iota = lax.broadcasted_iota(jnp.int32, (experts, rows), 0)
    chosen = jnp.zeros((experts, rows), jnp.float32)
    weight = jnp.zeros((experts, rows), jnp.float32)
    for choice in range(top_count):
        named = ids_ref[choice : choice + 1, :] == expert_iota
        chosen = jnp.where(named, 1.0, chosen)
        weight = jnp.where(named, route_weight_ref[choice : choice + 1, :], weight)
    earlier = jnp.where(
        lax.broadcasted_iota(jnp.int32, (rows, rows), 0)
        < lax.broadcasted_iota(jnp.int32, (rows, rows), 1),
        1.0,
        0.0,
    ).astype(jnp.bfloat16)
    before = jnp.dot(
        chosen.astype(jnp.bfloat16), earlier, preferred_element_type=jnp.float32
    )
    slot = jnp.where(chosen > 0.0, before, -1.0)
    slot_iota = lax.broadcasted_iota(jnp.int32, (capacity, rows), 0).astype(jnp.float32)
    for expert in range(experts):
        lines = slice(expert * capacity, (expert + 1) * capacity)
        taken = slot[expert : expert + 1, :] == slot_iota
        taken_ref[lines, :] = jnp.where(taken, 1.0, 0.0).astype(jnp.bfloat16)
        combine_ref[lines, :] = jnp.where(taken, weight[expert : expert + 1, :], 0.0)


def layer_kernel(
    peers,
    capacity,
    group_channels,
    residual_ref,
    ids_ref,
    route_weight_ref,
    mix_gain_ref,
    decay_ref,
    frequency_ref,
    step_ref,
    passthrough_ref,
    out_gain_ref,
    ffn_gain_ref,
    state_hbm,
    in_hbm,
    push_hbm,
    read_hbm,
    out_hbm,
    gate_hbm,
    up_hbm,
    down_hbm,
    out_ref,
    state_v,
    in_v,
    push_v,
    read_v,
    out_v,
    residual_other,
    mixer_own,
    mixer_other,
    after_ref,
    transition_ref,
    taken_ref,
    combine_ref,
    buffer_ref,
    gate_w,
    up_w,
    down_w,
    rows_own,
    rows_other,
    flat_own,
    flat_other,
    activation,
    part_send,
    part_recv,
    part_own,
    back_send,
    back_recv,
    weight_sem,
    mixer_sem,
    swap_send_sem,
    swap_recv_sem,
    go_send_sem,
    go_recv_sem,
    pair_send_sem,
    pair_recv_sem,
    part_send_sem,
    part_recv_sem,
    back_send_sem,
    back_recv_sem,
):
    me = lax.axis_index("ep")
    core = lax.axis_index("tp")
    half_width = residual_ref.shape[1]
    hidden = gate_w.shape[1]
    tile = 256
    mixer_copies = [
        pltpu.make_async_copy(source, target, mixer_sem.at[place])
        for place, (source, target) in enumerate(
            (
                (in_hbm, in_v),
                (push_hbm, push_v),
                (state_hbm, state_v),
                (read_hbm, read_v),
                (out_hbm, out_v),
            )
        )
    ]
    weights = [
        pltpu.make_async_copy(gate_hbm, gate_w, weight_sem.at[0]),
        pltpu.make_async_copy(up_hbm, up_w, weight_sem.at[1]),
        pltpu.make_async_copy(down_hbm, down_w, weight_sem.at[2]),
    ]
    for copy in mixer_copies:
        copy.start()
    barrier = pltpu.get_barrier_semaphore()
    for offset in range(1, peers):
        pl.semaphore_signal(
            barrier,
            inc=1,
            device_id=(peer_of(me, offset), core),
            device_id_type=pl.DeviceIdType.MESH,
        )
    pl.semaphore_signal(
        barrier, inc=1, device_id=(me, 1 - core), device_id_type=pl.DeviceIdType.MESH
    )
    fill_transition(decay_ref, frequency_ref, step_ref, transition_ref)
    fill_routes(capacity, ids_ref, route_weight_ref, taken_ref, combine_ref)
    pl.semaphore_wait(barrier, peers)

    def remote(source, target, send_sem, recv_sem, ep_index, tp_index):
        return pltpu.make_async_remote_copy(
            src_ref=source,
            dst_ref=target,
            send_sem=send_sem,
            recv_sem=recv_sem,
            device_id=(ep_index, tp_index),
            device_id_type=pl.DeviceIdType.MESH,
        )

    own_start = pl.multiple_of(core * half_width, half_width)
    other_start = pl.multiple_of((1 - core) * half_width, half_width)
    own_columns = pl.ds(own_start, half_width)
    other_columns = pl.ds(other_start, half_width)
    narrow = jnp.bfloat16
    swap_rows = remote(
        residual_ref, residual_other, swap_send_sem.at[0], swap_recv_sem.at[0], me, 1 - core
    )
    swap_rows.start()
    start_rows = residual_ref[...].astype(jnp.float32)
    gained = (start_rows * mix_gain_ref[:, own_columns]).astype(narrow)
    squares = row_squares(start_rows)
    mixer_copies[0].wait()
    channels_sum = jnp.dot(gained, in_v[own_columns, :], preferred_element_type=jnp.float32)
    swap_rows.wait_recv()
    other_rows = residual_other[...].astype(jnp.float32)
    gained = (other_rows * mix_gain_ref[:, other_columns]).astype(narrow)
    squares = squares + row_squares(other_rows)
    channels_sum = channels_sum + jnp.dot(
        gained, in_v[other_columns, :], preferred_element_type=jnp.float32
    )
    channels = (channels_sum * lax.rsqrt(squares / (2 * half_width) + epsilon)).astype(narrow)
    for copy in weights:
        copy.start()

    mixer_width = channels.shape[1]
    entries = push_v.shape[2]
    wide = 128
    groups = wide // group_channels
    block = groups * entries
    shape = (wide, block)
    inside = (
        lax.broadcasted_iota(jnp.int32, shape, 0) // group_channels
        == lax.broadcasted_iota(jnp.int32, shape, 1) // entries
    )

    def block_diagonal(source, part, start):
        values = source[part, start : start + wide, :]
        return jnp.where(inside, jnp.concatenate([values] * groups, axis=1), 0.0).astype(narrow)

    for copy in mixer_copies[1:4]:
        copy.wait()
    for place in range(mixer_width // wide):
        start = place * wide
        states = slice(place * block, (place + 1) * block)
        inputs = channels[:, start : start + wide]
        raw_real = jnp.dot(
            inputs, block_diagonal(push_v, 0, start), preferred_element_type=jnp.float32
        )
        raw_imag = jnp.dot(
            inputs, block_diagonal(push_v, 1, start), preferred_element_type=jnp.float32
        )
        bar_real, bar_imag = transition_ref[0:1, states], transition_ref[1:2, states]
        coef_real, coef_imag = transition_ref[2:3, states], transition_ref[3:4, states]
        old_real, old_imag = state_v[0, :, states], state_v[1, :, states]
        new_real = (
            bar_real * old_real - bar_imag * old_imag + coef_real * raw_real - coef_imag * raw_imag
        )
        new_imag = (
            bar_real * old_imag + bar_imag * old_real + coef_real * raw_imag + coef_imag * raw_real
        )
        state_v[0, :, states] = new_real
        state_v[1, :, states] = new_imag
        transposed = (((1,), (1,)), ((), ()))
        mixed = (
            lax.dot_general(
                new_real.astype(narrow),
                block_diagonal(read_v, 0, start),
                transposed,
                preferred_element_type=jnp.float32,
            )
            - lax.dot_general(
                new_imag.astype(narrow),
                block_diagonal(read_v, 1, start),
                transposed,
                preferred_element_type=jnp.float32,
            )
            + passthrough_ref[:, start : start + wide] * inputs.astype(jnp.float32)
        )
        mixer_own[:, start : start + wide] = gelu_tanh(mixed).astype(narrow)
    swap_mixed = remote(
        mixer_own, mixer_other, swap_send_sem.at[1], swap_recv_sem.at[1], me, 1 - core
    )
    swap_mixed.start()
    own_channels = pl.ds(pl.multiple_of(core * mixer_width, mixer_width), mixer_width)
    other_channels = pl.ds(pl.multiple_of((1 - core) * mixer_width, mixer_width), mixer_width)
    mine = mixer_own[...].astype(jnp.float32)
    squares = row_squares(mine)
    mixer_copies[4].wait()
    projected = jnp.dot(
        (mine * out_gain_ref[:, own_channels]).astype(narrow),
        out_v[own_channels, :],
        preferred_element_type=jnp.float32,
    )
    swap_mixed.wait_recv()
    others = mixer_other[...].astype(jnp.float32)
    squares = squares + row_squares(others)
    projected = projected + jnp.dot(
        (others * out_gain_ref[:, other_channels]).astype(narrow),
        out_v[other_channels, :],
        preferred_element_type=jnp.float32,
    )
    after_rows = (
        start_rows + projected * lax.rsqrt(squares / (2 * mixer_width) + epsilon)
    ).astype(narrow)
    after_ref[...] = after_rows
    quarter = peers // 4
    for place in range(4):
        slots = slice(place * quarter * capacity, (place + 1) * quarter * capacity)
        buffer_ref[place * quarter : (place + 1) * quarter] = (
            jnp.dot(taken_ref[slots, :], after_rows, preferred_element_type=jnp.float32)
            .reshape(quarter, capacity, half_width)
            .astype(narrow)
        )

    half = peers // 2
    outward = {}
    middle = half + half // 2
    chunks = ((half, middle), (0, half), (middle, peers))
    for offset in [one for span in chunks for one in range(*span) if one]:
        peer = peer_of(me, offset)
        outward[offset] = remote(
            buffer_ref.at[peer],
            rows_own.at[offset],
            go_send_sem.at[offset],
            go_recv_sem.at[offset],
            peer,
            core,
        )
        outward[offset].start()
    rows_own[0] = buffer_ref[me]
    back = {}
    parts = []
    pairs = {}
    for chunk, (first, last) in enumerate(chunks):
        count = (last - first) * capacity
        for offset in range(first, last):
            if offset:
                outward[offset].wait_recv()
            source = rows_own.at[offset] if offset else buffer_ref.at[me]
            pairs[offset] = remote(
                source,
                rows_other.at[offset],
                pair_send_sem.at[offset],
                pair_recv_sem.at[offset],
                me,
                1 - core,
            )
            pairs[offset].start()
        own_rows = (
            rows_own[first:last]
            .astype(jnp.float32)
            .reshape(count, half_width)
        )
        for offset in range(first, last):
            pairs[offset].wait_recv()
        other_half = (
            rows_other[first:last]
            .astype(jnp.float32)
            .reshape(count, half_width)
        )
        row_scale = lax.rsqrt(
            (row_squares(own_rows) + row_squares(other_half)) / (2 * half_width) + epsilon
        )
        flat_own[0:count] = (own_rows * row_scale * ffn_gain_ref[:, own_columns]).astype(narrow)
        flat_other[0:count] = (other_half * row_scale * ffn_gain_ref[:, other_columns]).astype(narrow)
        if chunk == 0:
            weights[0].wait()
            weights[1].wait()

        def hidden_tile(step, carry, count=count):
            columns = pl.ds(pl.multiple_of(step * tile, tile), tile)

            def both(weight):
                return jnp.dot(
                    flat_own[0:count],
                    weight[pl.ds(own_start, half_width), columns],
                    preferred_element_type=jnp.float32,
                ) + jnp.dot(
                    flat_other[0:count],
                    weight[pl.ds(other_start, half_width), columns],
                    preferred_element_type=jnp.float32,
                )

            gated = jnp.minimum(both(gate_w), clamp_limit)
            raised = jnp.clip(both(up_w), -clamp_limit, clamp_limit) + 1.0
            activation[0:count, columns] = (
                raised * gated * (1.0 / (1.0 + jnp.exp(-swish_alpha * gated)))
            ).astype(jnp.bfloat16)
            return carry

        lax.fori_loop(0, hidden // tile, hidden_tile, 0)
        if chunk == 0:
            weights[2].wait()

        def down_tiles(start, target):
            def down_tile(step, carry, count=count):
                columns = pl.ds(pl.multiple_of(step * tile, tile), tile)
                source = pl.ds(pl.multiple_of(start + step * tile, tile), tile)
                target[0:count, columns] = jnp.dot(
                    activation[0:count], down_w[:, source], preferred_element_type=jnp.float32
                ).astype(jnp.bfloat16)
                return carry

            lax.fori_loop(0, half_width // tile, down_tile, 0)

        down_tiles(other_start, part_send.at[chunk])
        parts.append(
            remote(
                part_send.at[chunk, pl.ds(0, count)],
                part_recv.at[chunk, pl.ds(0, count)],
                part_send_sem.at[chunk],
                part_recv_sem.at[chunk],
                me,
                1 - core,
            )
        )
        parts[chunk].start()
        down_tiles(own_start, part_own)
        parts[chunk].wait_recv()
        back_send[first:last] = (
            (part_own[0:count].astype(jnp.float32) + part_recv[chunk, 0:count].astype(jnp.float32))
            .reshape(last - first, capacity, half_width)
            .astype(jnp.bfloat16)
        )
        for offset in range(first, last):
            if offset == 0:
                back_recv[me] = back_send[0]
                continue
            peer = peer_of(me, offset)
            back[offset] = remote(
                back_send.at[offset],
                back_recv.at[me],
                back_send_sem.at[offset],
                back_recv_sem.at[offset],
                peer,
                core,
            )
            back[offset].start()
    for offset in range(1, peers):
        back[offset].wait_recv()
    returned = (
        back_recv[...]
        .astype(jnp.float32)
        .reshape(peers * capacity, half_width)
        .astype(jnp.bfloat16)
    )
    high = combine_ref[...].astype(jnp.bfloat16)
    low = (combine_ref[...] - high.astype(jnp.float32)).astype(jnp.bfloat16)
    over_slots = (((0,), (0,)), ((), ()))
    expert_sum = lax.dot_general(
        high, returned, over_slots, preferred_element_type=jnp.float32
    ) + lax.dot_general(low, returned, over_slots, preferred_element_type=jnp.float32)
    out_ref[...] = (after_ref[...].astype(jnp.float32) + expert_sum).astype(jnp.bfloat16)
    for offset in range(1, peers):
        outward[offset].wait_send()
        back[offset].wait_send()
    for offset in range(peers):
        pairs[offset].wait_send()
    for copy in parts:
        copy.wait_send()
    swap_rows.wait_send()
    swap_mixed.wait_send()


def layer_call(group_channels, peers, capacity, residual, *operands):
    state, in_proj, push_map, read_map, out_proj, w_gate, w_up, w_down = operands[9:]
    half_width = residual.shape[1]
    rows = peers // 2 * capacity
    narrow = jnp.bfloat16
    blocks = pltpu.VMEM((peers, capacity, half_width), narrow)
    flat = pltpu.VMEM((rows, half_width), narrow)
    mixer = pltpu.VMEM((residual.shape[0], in_proj.shape[1]), narrow)
    dma = pltpu.SemaphoreType.DMA
    vmem = pl.BlockSpec(memory_space=pltpu.VMEM)
    anywhere = pl.BlockSpec(memory_space=pl.ANY)
    return pl.pallas_call(
        functools.partial(layer_kernel, peers, capacity, group_channels),
        out_shape=(
            pltpu.VMEM(residual.shape, narrow),
            pltpu.VMEM(state.shape, jnp.float32),
        ),
        in_specs=[vmem] * 10 + [anywhere] * 8,
        out_specs=(vmem, vmem),
        scratch_shapes=[
            pltpu.VMEM(in_proj.shape, narrow),
            pltpu.VMEM(push_map.shape, jnp.float32),
            pltpu.VMEM(read_map.shape, jnp.float32),
            pltpu.VMEM(out_proj.shape, narrow),
            pltpu.VMEM(residual.shape, narrow),
            mixer,
            mixer,
            pltpu.VMEM(residual.shape, narrow),
            pltpu.VMEM((4, state.shape[2]), jnp.float32),
            pltpu.VMEM((peers * capacity, residual.shape[0]), narrow),
            pltpu.VMEM((peers * capacity, residual.shape[0]), jnp.float32),
            blocks,
            pltpu.VMEM(w_gate.shape, narrow),
            pltpu.VMEM(w_up.shape, narrow),
            pltpu.VMEM(w_down.shape, narrow),
            blocks,
            blocks,
            flat,
            flat,
            pltpu.VMEM((rows, w_gate.shape[1]), narrow),
            pltpu.VMEM((3, rows, half_width), narrow),
            pltpu.VMEM((3, rows, half_width), narrow),
            flat,
            blocks,
            blocks,
            dma((3,)),
            dma((5,)),
            dma((2,)),
            dma((2,)),
            dma((peers,)),
            dma((peers,)),
            dma((peers,)),
            dma((peers,)),
            dma((3,)),
            dma((3,)),
            dma((peers,)),
            dma((peers,)),
        ],
        compiler_params=pltpu.CompilerParams(
            collective_id=0, has_side_effects=True, vmem_limit_bytes=56 * 1024 * 1024
        ),
    )(residual, *operands)


def local(
    residual,
    route_ids,
    route_weights,
    carried_state,
    mix_gain,
    in_proj,
    decay_rate,
    frequency,
    step_size,
    input_map,
    output_matrix,
    passthrough_scale,
    out_gain,
    out_proj,
    ffn_gain,
    w_gate,
    w_up,
    w_down,
):
    row_count, half_width = residual.shape
    top_count = route_ids.shape[1]
    local_experts = w_gate.shape[0]
    peer_count = lax.axis_size("ep")
    expert_count = local_experts * peer_count
    capacity = max(2, 3 * row_count * top_count // (2 * expert_count))
    capacity = -(-capacity // 8) * 8
    push_map = jnp.swapaxes(input_map, 2, 3).reshape(2, -1, input_map.shape[2])
    read_map = output_matrix.reshape(2, -1, output_matrix.shape[3])
    updated, new_state = layer_call(
        input_map.shape[3],
        peer_count,
        capacity,
        residual,
        route_ids.T,
        route_weights.T,
        mix_gain[None, :],
        decay_rate,
        frequency,
        step_size[None, :],
        passthrough_scale[None, :],
        out_gain[None, :],
        ffn_gain[None, :],
        carried_state,
        in_proj,
        push_map,
        read_map,
        out_proj,
        w_gate[0],
        w_up[0],
        w_down[0],
    )
    return (updated, new_state)


def solution(mesh):
    placed = (
        P("ep", "tp"),
        P("ep", None),
        P("ep", None),
        P(None, "ep", "tp"),
        P(),
        P(None, "tp"),
        P("tp", None),
        P("tp", None),
        P("tp"),
        P(None, "tp", None, None),
        P(None, "tp", None, None),
        P("tp"),
        P(),
        P(None, "tp"),
        P(),
        P("ep", None, "tp"),
        P("ep", None, "tp"),
        P("ep", "tp", None),
    )
    return jax.shard_map(
        local,
        mesh=mesh,
        in_specs=placed,
        out_specs=(P("ep", "tp"), P(None, "ep", "tp")),
        check_vma=False,
    )
```

```python
import functools
import jax
import jax.numpy as jnp
from jax import lax
from jax.experimental import pallas as pl
from jax.experimental.pallas import tpu as pltpu
from jax.sharding import PartitionSpec as P

epsilon = 1e-06
clamp_limit = 7.0
swish_alpha = 1.702


def discretize(decay_rate, frequency, step_size):
    rate_real = -decay_rate
    time_step = step_size
    magnitude = jnp.exp(rate_real * time_step)
    phase_angle = frequency * time_step
    bar_real = magnitude * jnp.cos(phase_angle)
    bar_imag = magnitude * jnp.sin(phase_angle)
    denominator = rate_real * rate_real + frequency * frequency
    shifted = bar_real - 1.0
    coef_real = (shifted * rate_real + bar_imag * frequency) / denominator
    coef_imag = (bar_imag * rate_real - shifted * frequency) / denominator
    return (bar_real, bar_imag, coef_real, coef_imag)


def peer_of(index, offset):
    out = index
    bit = 1
    while bit <= offset:
        if offset & bit:
            out = out + bit * (1 - 2 * ((index // bit) % 2))
        bit *= 2
    return out


def gelu_tanh(value):
    inner = 0.7978845608028654 * (value + 0.044715 * value * value * value)
    return 0.5 * value * (1.0 + jnp.tanh(inner))


def row_squares(value):
    return jnp.sum(value * value, axis=1, keepdims=True)


def fill_transition(decay_ref, frequency_ref, step_ref, transition_ref):
    groups, entries = decay_ref.shape
    diagonal = lax.broadcasted_iota(jnp.int32, (groups, groups), 0) == lax.broadcasted_iota(
        jnp.int32, (groups, groups), 1
    )
    steps = jnp.sum(jnp.where(diagonal, step_ref[...], 0.0), axis=1, keepdims=True)
    shape = (groups, groups * entries)
    inside = (
        lax.broadcasted_iota(jnp.int32, shape, 0)
        == lax.broadcasted_iota(jnp.int32, shape, 1) // entries
    )
    for place, term in enumerate(discretize(decay_ref[...], frequency_ref[...], steps)):
        spread = jnp.concatenate([term] * groups, axis=1)
        transition_ref[place : place + 1, :] = jnp.sum(
            jnp.where(inside, spread, 0.0), axis=0, keepdims=True
        )


def fill_routes(capacity, route, experts, taken_ref, combine_ref):
    top_count = route.shape[0] // 2
    count, rows = experts.shape
    chosen = jnp.zeros((count, rows), jnp.float32)
    weight = jnp.zeros((count, rows), jnp.float32)
    for choice in range(top_count):
        named = route[choice : choice + 1, :] == experts
        chosen = jnp.where(named, 1.0, chosen)
        weight = jnp.where(named, route[top_count + choice : top_count + choice + 1, :], weight)
    earlier = jnp.where(
        lax.broadcasted_iota(jnp.int32, (rows, rows), 0)
        < lax.broadcasted_iota(jnp.int32, (rows, rows), 1),
        1.0,
        0.0,
    ).astype(jnp.bfloat16)
    before = jnp.dot(
        chosen.astype(jnp.bfloat16), earlier, preferred_element_type=jnp.float32
    )
    slot = jnp.where(chosen > 0.0, before, -1.0)
    slot_iota = lax.broadcasted_iota(jnp.int32, (capacity, rows), 0).astype(jnp.float32)
    for expert in range(count):
        lines = slice(expert * capacity, (expert + 1) * capacity)
        taken = slot[expert : expert + 1, :] == slot_iota
        taken_ref[lines, :] = jnp.where(taken, 1.0, 0.0).astype(jnp.bfloat16)
        combine_ref[lines, :] = jnp.where(taken, weight[expert : expert + 1, :], 0.0)


def layer_kernel(
    floors,
    peers,
    capacity,
    group_channels,
    residual_ref,
    ids_ref,
    route_weight_ref,
    mix_gain_ref,
    decay_ref,
    frequency_ref,
    step_ref,
    passthrough_ref,
    out_gain_ref,
    ffn_gain_ref,
    state_hbm,
    in_hbm,
    push_hbm,
    read_hbm,
    out_hbm,
    gate_hbm,
    up_hbm,
    down_hbm,
    out_ref,
    state_v,
    in_v,
    push_v,
    read_v,
    out_v,
    residual_other,
    mixer_other,
    after_ref,
    transition_ref,
    routes,
    taken_ref,
    combine_ref,
    line_rows,
    line_mixed,
    row_buffer,
    mixed_buffer,
    row_slots,
    mixed_slots,
    mixed_other,
    mixed_flat,
    after_own,
    after_other,
    gate_w,
    up_w,
    down_w,
    flat,
    activation,
    part_send,
    part_recv,
    part_own,
    back_send,
    back_recv,
    sum_send,
    sum_recv,
    weight_sem,
    mixer_sem,
    swap_send_sem,
    swap_recv_sem,
    line_send_sem,
    line_recv_sem,
    pair_send_sem,
    pair_recv_sem,
    plane_send_sem,
    plane_recv_sem,
):
    me = lax.axis_index("ep")
    core = lax.axis_index("tp")
    half_width = residual_ref.shape[1]
    hidden = gate_w.shape[1]
    tile = 1024
    mixer_copies = [
        pltpu.make_async_copy(source, target, mixer_sem.at[place])
        for place, (source, target) in enumerate(
            (
                (in_hbm, in_v),
                (push_hbm, push_v),
                (state_hbm, state_v),
                (read_hbm, read_v),
                (out_hbm, out_v),
            )
        )
    ]
    weights = [
        pltpu.make_async_copy(gate_hbm, gate_w, weight_sem.at[0]),
        pltpu.make_async_copy(up_hbm, up_w, weight_sem.at[1]),
        pltpu.make_async_copy(down_hbm, down_w, weight_sem.at[2]),
    ]
    for copy in mixer_copies:
        copy.start()
    plane = peers // floors
    barrier = pltpu.get_barrier_semaphore()
    greeted = [one for one in range(1, plane)] + [one * plane for one in range(1, floors)]
    for offset in greeted:
        pl.semaphore_signal(
            barrier,
            inc=1,
            device_id=(peer_of(me, offset), core),
            device_id_type=pl.DeviceIdType.MESH,
        )
    pl.semaphore_signal(
        barrier, inc=1, device_id=(me, 1 - core), device_id_type=pl.DeviceIdType.MESH
    )
    row_count = residual_ref.shape[0]
    shape = (plane, row_count)
    experts = (
        me // plane * plane
        + jnp.bitwise_xor(lax.broadcasted_iota(jnp.int32, shape, 0), me % plane)
    ).astype(jnp.float32)
    routes[0] = jnp.concatenate(
        [ids_ref[...].astype(jnp.float32), route_weight_ref[...]], axis=0
    )
    fill_transition(decay_ref, frequency_ref, step_ref, transition_ref)
    fill_routes(capacity, routes[0], experts, taken_ref.at[0], combine_ref.at[0])
    pl.semaphore_wait(barrier, len(greeted) + 1)

    def remote(source, target, send_sem, recv_sem, ep_index, tp_index):
        return pltpu.make_async_remote_copy(
            src_ref=source,
            dst_ref=target,
            send_sem=send_sem,
            recv_sem=recv_sem,
            device_id=(ep_index, tp_index),
            device_id_type=pl.DeviceIdType.MESH,
        )

    own_start = pl.multiple_of(core * half_width, half_width)
    other_start = pl.multiple_of((1 - core) * half_width, half_width)
    own_columns = pl.ds(own_start, half_width)
    other_columns = pl.ds(other_start, half_width)
    narrow = jnp.bfloat16
    swap_rows = remote(
        residual_ref, residual_other, swap_send_sem.at[0], swap_recv_sem.at[0], me, 1 - core
    )
    swap_rows.start()
    line_copies = {}
    kinds = {"route": 0, "rows": 1, "mixed": 2, "sum": 3}

    def to_line(kind, source, target, step, toward=None):
        line_copies[kind, step] = remote(
            source,
            target,
            line_send_sem.at[kinds[kind], step],
            line_recv_sem.at[kinds[kind], step],
            peer_of(me, (toward or step) * plane),
            core,
        )
        line_copies[kind, step].start()

    passed_on = {2: (3, 1)} if floors == 4 else {}
    outer = list(range(floors - 1, 0, -1))
    for step in outer:
        to_line("route", routes.at[0], routes.at[step], step)
    for step in outer:
        if step not in passed_on:
            to_line("rows", residual_ref, line_rows.at[step], step)
    plane_copies = {}
    plane_kinds = {"rows": 0, "mixed": 1, "back": 2}

    def to_plane(kind, step, source, target):
        for turn in range(1, plane):
            plane_copies[kind, step, turn] = remote(
                source.at[step, turn],
                target.at[step, turn],
                plane_send_sem.at[plane_kinds[kind], step, turn],
                plane_recv_sem.at[plane_kinds[kind], step, turn],
                peer_of(me, turn),
                core,
            )
            plane_copies[kind, step, turn].start()
        target[step, 0] = source[step, 0]

    def from_plane(kind, step):
        for turn in range(1, plane):
            plane_copies[kind, step, turn].wait_recv()

    def hand_out(kind, step, values, buffer, target):
        buffer[step] = (
            jnp.dot(taken_ref[step], values, preferred_element_type=jnp.float32)
            .reshape(plane, capacity, values.shape[1])
            .astype(jnp.bfloat16)
        )
        to_plane(kind, step, buffer, target)

    start_rows = residual_ref[...].astype(jnp.float32)
    gained = (start_rows * mix_gain_ref[:, own_columns]).astype(narrow)
    squares = row_squares(start_rows)
    mixer_copies[0].wait()
    channels_sum = jnp.dot(gained, in_v[own_columns, :], preferred_element_type=jnp.float32)
    hand_out("rows", 0, residual_ref[...], row_buffer, row_slots)
    swap_rows.wait_recv()
    other_rows = residual_other[...].astype(jnp.float32)
    gained = (other_rows * mix_gain_ref[:, other_columns]).astype(narrow)
    squares = squares + row_squares(other_rows)
    channels_sum = channels_sum + jnp.dot(
        gained, in_v[other_columns, :], preferred_element_type=jnp.float32
    )
    channels = (channels_sum * lax.rsqrt(squares / (2 * half_width) + epsilon)).astype(narrow)
    for copy in weights:
        copy.start()

    mixer_width = channels.shape[1]
    entries = push_v.shape[2]
    wide = 128
    groups = wide // group_channels
    block = groups * entries
    shape = (wide, block)
    inside = (
        lax.broadcasted_iota(jnp.int32, shape, 0) // group_channels
        == lax.broadcasted_iota(jnp.int32, shape, 1) // entries
    )

    def block_diagonal(source, part, start):
        values = source[part, start : start + wide, :]
        return jnp.where(inside, jnp.concatenate([values] * groups, axis=1), 0.0).astype(narrow)

    for copy in mixer_copies[1:4]:
        copy.wait()
    for place in range(mixer_width // wide):
        start = place * wide
        states = slice(place * block, (place + 1) * block)
        inputs = channels[:, start : start + wide]
        raw_real = jnp.dot(
            inputs, block_diagonal(push_v, 0, start), preferred_element_type=jnp.float32
        )
        raw_imag = jnp.dot(
            inputs, block_diagonal(push_v, 1, start), preferred_element_type=jnp.float32
        )
        bar_real, bar_imag = transition_ref[0:1, states], transition_ref[1:2, states]
        coef_real, coef_imag = transition_ref[2:3, states], transition_ref[3:4, states]
        old_real, old_imag = state_v[0, :, states], state_v[1, :, states]
        new_real = (
            bar_real * old_real - bar_imag * old_imag + coef_real * raw_real - coef_imag * raw_imag
        )
        new_imag = (
            bar_real * old_imag + bar_imag * old_real + coef_real * raw_imag + coef_imag * raw_real
        )
        state_v[0, :, states] = new_real
        state_v[1, :, states] = new_imag
        transposed = (((1,), (1,)), ((), ()))
        mixed = (
            lax.dot_general(
                new_real.astype(narrow),
                block_diagonal(read_v, 0, start),
                transposed,
                preferred_element_type=jnp.float32,
            )
            - lax.dot_general(
                new_imag.astype(narrow),
                block_diagonal(read_v, 1, start),
                transposed,
                preferred_element_type=jnp.float32,
            )
            + passthrough_ref[:, start : start + wide] * inputs.astype(jnp.float32)
        )
        line_mixed[0, :, start : start + wide] = gelu_tanh(mixed).astype(narrow)
    for step in outer:
        to_line("mixed", line_mixed.at[0], line_mixed.at[step], step)
    swap_mixed = remote(
        line_mixed.at[0], mixer_other, swap_send_sem.at[1], swap_recv_sem.at[1], me, 1 - core
    )
    swap_mixed.start()
    hand_out("mixed", 0, line_mixed[0], mixed_buffer, mixed_slots)
    own_channels = pl.ds(pl.multiple_of(core * mixer_width, mixer_width), mixer_width)
    other_channels = pl.ds(pl.multiple_of((1 - core) * mixer_width, mixer_width), mixer_width)

    def after_mixer(rows, mine, others):
        count = rows.shape[0]
        squares = row_squares(mine) + row_squares(others)
        mixed_flat[0:count, own_channels] = (mine * out_gain_ref[:, own_channels]).astype(narrow)
        mixed_flat[0:count, other_channels] = (
            others * out_gain_ref[:, other_channels]
        ).astype(narrow)
        projected = jnp.dot(
            mixed_flat[0:count], out_v[...], preferred_element_type=jnp.float32
        )
        return (rows + projected * lax.rsqrt(squares / (2 * mixer_width) + epsilon)).astype(
            narrow
        )

    def relay_rows(step):
        line_copies["route", step].wait_recv()
        fill_routes(capacity, routes[step], experts, taken_ref.at[step], combine_ref.at[step])
        line_copies["rows", step].wait_recv()
        for late, (source, toward) in passed_on.items():
            if source == step:
                to_line("rows", line_rows.at[source], line_rows.at[late], late, toward)
        hand_out("rows", step, line_rows[step], row_buffer, row_slots)

    def relay_mixed(step):
        line_copies["mixed", step].wait_recv()
        hand_out("mixed", step, line_mixed[step], mixed_buffer, mixed_slots)

    prompt = [step for step in range(1, floors) if step not in passed_on]
    for step in prompt:
        relay_rows(step)
    mixer_copies[4].wait()
    swap_mixed.wait_recv()
    after_ref[...] = after_mixer(
        start_rows, line_mixed[0].astype(jnp.float32), mixer_other[...].astype(jnp.float32)
    )
    for step in prompt:
        relay_mixed(step)
    for step in passed_on:
        relay_rows(step)
        relay_mixed(step)

    pairs = {}
    slots = plane * capacity

    def to_pair(kind, place, source, target):
        pairs[kind, place] = remote(
            source,
            target,
            pair_send_sem.at[kind, place],
            pair_recv_sem.at[kind, place],
            me,
            1 - core,
        )
        pairs[kind, place].start()

    def share_mixed(step):
        from_plane("mixed", step)
        to_pair(0, step, mixed_slots.at[step], mixed_other.at[step])

    def project(step):
        pairs[0, step].wait_recv()
        from_plane("rows", step)
        after_own[step] = after_mixer(
            row_slots[step].astype(jnp.float32).reshape(slots, half_width),
            mixed_slots[step].astype(jnp.float32).reshape(slots, mixer_width),
            mixed_other[step].astype(jnp.float32).reshape(slots, mixer_width),
        )
        to_pair(1, step, after_own.at[step], after_other.at[step])

    def apply_expert(chunk, first, last):
        count = (last - first) * slots
        for step in range(first, last):
            pairs[1, step].wait_recv()
        own_rows = after_own[first:last].astype(jnp.float32).reshape(count, half_width)
        other_half = after_other[first:last].astype(jnp.float32).reshape(count, half_width)
        row_scale = lax.rsqrt(
            (row_squares(own_rows) + row_squares(other_half)) / (2 * half_width) + epsilon
        )
        flat[0:count, own_columns] = (own_rows * row_scale * ffn_gain_ref[:, own_columns]).astype(
            narrow
        )
        flat[0:count, other_columns] = (
            other_half * row_scale * ffn_gain_ref[:, other_columns]
        ).astype(narrow)
        if chunk == 0:
            weights[0].wait()
            weights[1].wait()
        for start in range(0, hidden, tile):
            columns = slice(start, start + tile)

            def both(weight):
                return jnp.dot(
                    flat[0:count], weight[:, columns], preferred_element_type=jnp.float32
                )

            gated = jnp.minimum(both(gate_w), clamp_limit)
            raised = jnp.clip(both(up_w), -clamp_limit, clamp_limit) + 1.0
            activation[0:count, columns] = (
                raised * gated * (1.0 / (1.0 + jnp.exp(-swish_alpha * gated)))
            ).astype(jnp.bfloat16)
        if chunk == 0:
            weights[2].wait()
        part_send[chunk, 0:count] = jnp.dot(
            activation[0:count], down_w[:, other_columns], preferred_element_type=jnp.float32
        ).astype(jnp.bfloat16)
        to_pair(
            2,
            chunk,
            part_send.at[chunk, pl.ds(0, count)],
            part_recv.at[chunk, pl.ds(0, count)],
        )
        part_own[0:count] = jnp.dot(
            activation[0:count], down_w[:, own_columns], preferred_element_type=jnp.float32
        ).astype(jnp.bfloat16)
        pairs[2, chunk].wait_recv()
        back_send[first:last] = (
            (part_own[0:count].astype(jnp.float32) + part_recv[chunk, 0:count].astype(jnp.float32))
            .reshape(last - first, plane, capacity, half_width)
            .astype(jnp.bfloat16)
        )
        for step in range(last - 1, first - 1, -1):
            to_plane("back", step, back_send, back_recv)

    over_slots = (((0,), (0,)), ((), ()))

    def weigh(step):
        from_plane("back", step)
        returned = (
            back_recv[step].astype(jnp.float32).reshape(slots, half_width).astype(jnp.bfloat16)
        )
        high = combine_ref[step].astype(jnp.bfloat16)
        low = (combine_ref[step] - high.astype(jnp.float32)).astype(jnp.bfloat16)
        return lax.dot_general(
            high, returned, over_slots, preferred_element_type=jnp.float32
        ) + lax.dot_general(low, returned, over_slots, preferred_element_type=jnp.float32)

    def send_sum(step):
        sum_send[step] = weigh(step).astype(jnp.bfloat16)
        to_line("sum", sum_send.at[step], sum_recv.at[step], step)

    near = max(1, floors // 2)
    chunks = [(step, step + 1) for step in range(floors - 1, near - 1, -1)] + [(0, near)]
    for step in outer + [0]:
        share_mixed(step)
    for step in outer + [0]:
        project(step)
    for chunk, (first, last) in enumerate(chunks):
        apply_expert(chunk, first, last)
        if chunk:
            for step in range(chunks[chunk - 1][1] - 1, chunks[chunk - 1][0] - 1, -1):
                send_sum(step)
    for step in range(near - 1, 0, -1):
        send_sum(step)
    total = after_ref[...].astype(jnp.float32) + weigh(0)
    for step in range(1, floors):
        line_copies["sum", step].wait_recv()
        total = total + sum_recv[step].astype(jnp.float32)
    out_ref[...] = total.astype(jnp.bfloat16)
    for group in (line_copies, plane_copies, pairs):
        for copy in group.values():
            copy.wait_send()
    swap_rows.wait_send()
    swap_mixed.wait_send()


def layer_call(floors, group_channels, peers, capacity, residual, *operands):
    state, in_proj, push_map, read_map, out_proj, w_gate, w_up, w_down = operands[9:]
    row_count, half_width = residual.shape
    channels = in_proj.shape[1]
    plane = peers // floors
    slots = plane * capacity
    near = max(1, floors // 2)
    chunk_count = floors - near + 1
    rows = near * slots
    narrow = jnp.bfloat16
    wide_blocks = pltpu.VMEM((floors, plane, capacity, half_width), narrow)
    thin_blocks = pltpu.VMEM((floors, plane, capacity, channels), narrow)
    dma = pltpu.SemaphoreType.DMA
    vmem = pl.BlockSpec(memory_space=pltpu.VMEM)
    anywhere = pl.BlockSpec(memory_space=pl.ANY)
    return pl.pallas_call(
        functools.partial(layer_kernel, floors, peers, capacity, group_channels),
        out_shape=(
            pltpu.VMEM(residual.shape, narrow),
            pltpu.VMEM(state.shape, jnp.float32),
        ),
        in_specs=[vmem] * 10 + [anywhere] * 8,
        out_specs=(vmem, vmem),
        scratch_shapes=[
            pltpu.VMEM(in_proj.shape, narrow),
            pltpu.VMEM(push_map.shape, jnp.float32),
            pltpu.VMEM(read_map.shape, jnp.float32),
            pltpu.VMEM(out_proj.shape, narrow),
            pltpu.VMEM(residual.shape, narrow),
            pltpu.VMEM((row_count, channels), narrow),
            pltpu.VMEM(residual.shape, narrow),
            pltpu.VMEM((4, state.shape[2]), jnp.float32),
            pltpu.VMEM((floors, 2 * operands[0].shape[0], row_count), jnp.float32),
            pltpu.VMEM((floors, slots, row_count), narrow),
            pltpu.VMEM((floors, slots, row_count), jnp.float32),
            pltpu.VMEM((floors, row_count, half_width), narrow),
            pltpu.VMEM((floors, row_count, channels), narrow),
            wide_blocks,
            thin_blocks,
            wide_blocks,
            thin_blocks,
            thin_blocks,
            pltpu.VMEM((max(slots, row_count), 2 * channels), narrow),
            pltpu.VMEM((floors, slots, half_width), narrow),
            pltpu.VMEM((floors, slots, half_width), narrow),
            pltpu.VMEM(w_gate.shape, narrow),
            pltpu.VMEM(w_up.shape, narrow),
            pltpu.VMEM(w_down.shape, narrow),
            pltpu.VMEM((rows, 2 * half_width), narrow),
            pltpu.VMEM((rows, w_gate.shape[1]), narrow),
            pltpu.VMEM((chunk_count, rows, half_width), narrow),
            pltpu.VMEM((chunk_count, rows, half_width), narrow),
            pltpu.VMEM((rows, half_width), narrow),
            wide_blocks,
            wide_blocks,
            pltpu.VMEM((floors, row_count, half_width), narrow),
            pltpu.VMEM((floors, row_count, half_width), narrow),
            dma((3,)),
            dma((5,)),
            dma((2,)),
            dma((2,)),
            dma((4, floors)),
            dma((4, floors)),
            dma((3, floors)),
            dma((3, floors)),
            dma((3, floors, plane)),
            dma((3, floors, plane)),
        ],
        compiler_params=pltpu.CompilerParams(
            collective_id=0, has_side_effects=True, vmem_limit_bytes=56 * 1024 * 1024
        ),
    )(residual, *operands)


def local(
    floors,
    residual,
    route_ids,
    route_weights,
    carried_state,
    mix_gain,
    in_proj,
    decay_rate,
    frequency,
    step_size,
    input_map,
    output_matrix,
    passthrough_scale,
    out_gain,
    out_proj,
    ffn_gain,
    w_gate,
    w_up,
    w_down,
):
    row_count, half_width = residual.shape
    top_count = route_ids.shape[1]
    local_experts = w_gate.shape[0]
    peer_count = lax.axis_size("ep")
    expert_count = local_experts * peer_count
    capacity = max(2, 3 * row_count * top_count // (2 * expert_count))
    capacity = -(-capacity // 8) * 8
    push_map = jnp.swapaxes(input_map, 2, 3).reshape(2, -1, input_map.shape[2])
    read_map = output_matrix.reshape(2, -1, output_matrix.shape[3])
    updated, new_state = layer_call(
        floors,
        input_map.shape[3],
        peer_count,
        capacity,
        residual,
        route_ids.T,
        route_weights.T,
        mix_gain[None, :],
        decay_rate,
        frequency,
        step_size[None, :],
        passthrough_scale[None, :],
        out_gain[None, :],
        ffn_gain[None, :],
        carried_state,
        in_proj,
        push_map,
        read_map,
        out_proj,
        w_gate[0],
        w_up[0],
        w_down[0],
    )
    return (updated, new_state)


def floor_count(mesh):
    heights = {getattr(device, "coords", (0, 0, 0))[2] for device in mesh.devices.flat}
    return len(heights)


def solution(mesh):
    placed = (
        P("ep", "tp"),
        P("ep", None),
        P("ep", None),
        P(None, "ep", "tp"),
        P(),
        P(None, "tp"),
        P("tp", None),
        P("tp", None),
        P("tp"),
        P(None, "tp", None, None),
        P(None, "tp", None, None),
        P("tp"),
        P(),
        P(None, "tp"),
        P(),
        P("ep", None, "tp"),
        P("ep", None, "tp"),
        P("ep", "tp", None),
    )
    return jax.shard_map(
        functools.partial(local, floor_count(mesh)),
        mesh=mesh,
        in_specs=placed,
        out_specs=(P("ep", "tp"), P(None, "ep", "tp")),
        check_vma=False,
    )
```

```python
import functools
import jax
import jax.numpy as jnp
from jax import lax
from jax.experimental import pallas as pl
from jax.experimental.pallas import tpu as pltpu
from jax.sharding import PartitionSpec as P

epsilon = 1e-06
clamp_limit = 7.0
swish_alpha = 1.702


def discretize(decay_rate, frequency, step_size):
    rate_real = -decay_rate
    time_step = step_size
    magnitude = jnp.exp(rate_real * time_step)
    phase_angle = frequency * time_step
    bar_real = magnitude * jnp.cos(phase_angle)
    bar_imag = magnitude * jnp.sin(phase_angle)
    denominator = rate_real * rate_real + frequency * frequency
    shifted = bar_real - 1.0
    coef_real = (shifted * rate_real + bar_imag * frequency) / denominator
    coef_imag = (bar_imag * rate_real - shifted * frequency) / denominator
    return (bar_real, bar_imag, coef_real, coef_imag)


def peer_of(index, offset):
    out = index
    bit = 1
    while bit <= offset:
        if offset & bit:
            out = out + bit * (1 - 2 * ((index // bit) % 2))
        bit *= 2
    return out


def gelu_tanh(value):
    inner = 0.7978845608028654 * (value + 0.044715 * value * value * value)
    return 0.5 * value * (1.0 + jnp.tanh(inner))


def row_squares(value):
    return jnp.sum(value * value, axis=1, keepdims=True)


def fill_transition(decay_ref, frequency_ref, step_ref, transition_ref):
    groups, entries = decay_ref.shape
    diagonal = lax.broadcasted_iota(jnp.int32, (groups, groups), 0) == lax.broadcasted_iota(
        jnp.int32, (groups, groups), 1
    )
    steps = jnp.sum(jnp.where(diagonal, step_ref[...], 0.0), axis=1, keepdims=True)
    shape = (groups, groups * entries)
    inside = (
        lax.broadcasted_iota(jnp.int32, shape, 0)
        == lax.broadcasted_iota(jnp.int32, shape, 1) // entries
    )
    for place, term in enumerate(discretize(decay_ref[...], frequency_ref[...], steps)):
        spread = jnp.concatenate([term] * groups, axis=1)
        transition_ref[place : place + 1, :] = jnp.sum(
            jnp.where(inside, spread, 0.0), axis=0, keepdims=True
        )


def fill_routes(capacity, me, ids_ref, route_weight_ref, taken_ref, combine_ref):
    top_count, rows = ids_ref.shape
    experts = taken_ref.shape[0] // capacity
    expert_iota = jnp.bitwise_xor(lax.broadcasted_iota(jnp.int32, (experts, rows), 0), me)
    chosen = jnp.zeros((experts, rows), jnp.float32)
    weight = jnp.zeros((experts, rows), jnp.float32)
    for choice in range(top_count):
        named = ids_ref[choice : choice + 1, :] == expert_iota
        chosen = jnp.where(named, 1.0, chosen)
        weight = jnp.where(named, route_weight_ref[choice : choice + 1, :], weight)
    earlier = jnp.where(
        lax.broadcasted_iota(jnp.int32, (rows, rows), 0)
        < lax.broadcasted_iota(jnp.int32, (rows, rows), 1),
        1.0,
        0.0,
    ).astype(jnp.bfloat16)
    before = jnp.dot(
        chosen.astype(jnp.bfloat16), earlier, preferred_element_type=jnp.float32
    )
    slot = jnp.where(chosen > 0.0, before, -1.0)
    slot_iota = lax.broadcasted_iota(jnp.int32, (capacity, rows), 0).astype(jnp.float32)
    for expert in range(experts):
        lines = slice(expert * capacity, (expert + 1) * capacity)
        taken = slot[expert : expert + 1, :] == slot_iota
        taken_ref[lines, :] = jnp.where(taken, 1.0, 0.0).astype(jnp.bfloat16)
        combine_ref[lines, :] = jnp.where(taken, weight[expert : expert + 1, :], 0.0)


def layer_kernel(
    peers,
    capacity,
    group_channels,
    residual_hbm,
    ids_hbm,
    route_weight_hbm,
    mix_gain_hbm,
    decay_hbm,
    frequency_hbm,
    step_hbm,
    passthrough_hbm,
    out_gain_hbm,
    ffn_gain_hbm,
    state_hbm,
    in_hbm,
    push_hbm,
    read_hbm,
    out_hbm,
    gate_hbm,
    up_hbm,
    down_hbm,
    out_ref,
    state_v,
    residual_ref,
    ids_ref,
    route_weight_ref,
    mix_gain_ref,
    decay_ref,
    frequency_ref,
    step_ref,
    passthrough_ref,
    out_gain_ref,
    ffn_gain_ref,
    in_v,
    push_v,
    read_v,
    out_v,
    residual_other,
    mixer_own,
    mixer_other,
    after_ref,
    transition_ref,
    taken_ref,
    combine_ref,
    buffer_ref,
    gate_w,
    up_w,
    down_w,
    rows_own,
    rows_other,
    flat,
    activation,
    part_send,
    part_recv,
    part_own,
    back_send,
    back_recv,
    small_sem,
    weight_sem,
    mixer_sem,
    swap_send_sem,
    swap_recv_sem,
    go_send_sem,
    go_recv_sem,
    pair_send_sem,
    pair_recv_sem,
    part_send_sem,
    part_recv_sem,
    back_send_sem,
    back_recv_sem,
):
    me = lax.axis_index("ep")
    core = lax.axis_index("tp")
    half_width = residual_hbm.shape[1]
    hidden = gate_w.shape[1]
    tile = 1024
    half_rows = residual_hbm.shape[1]
    first_half = pl.ds(pl.multiple_of(core * half_rows, half_rows), half_rows)
    second_half = pl.ds(pl.multiple_of((1 - core) * half_rows, half_rows), half_rows)
    small_copies = [
        pltpu.make_async_copy(source, target, small_sem.at[place])
        for place, (source, target) in enumerate(
            (
                (residual_hbm, residual_ref),
                (mix_gain_hbm, mix_gain_ref),
                (ids_hbm, ids_ref),
                (route_weight_hbm, route_weight_ref),
                (decay_hbm, decay_ref),
                (frequency_hbm, frequency_ref),
                (step_hbm, step_ref),
                (passthrough_hbm, passthrough_ref),
                (out_gain_hbm, out_gain_ref),
                (ffn_gain_hbm, ffn_gain_ref),
            )
        )
    ]
    mixer_copies = [
        pltpu.make_async_copy(source, target, mixer_sem.at[place])
        for place, (source, target) in enumerate(
            (
                (in_hbm.at[first_half], in_v.at[first_half]),
                (in_hbm.at[second_half], in_v.at[second_half]),
                (push_hbm, push_v),
                (state_hbm, state_v),
                (read_hbm, read_v),
                (out_hbm, out_v),
            )
        )
    ]
    weights = [
        pltpu.make_async_copy(gate_hbm, gate_w, weight_sem.at[0]),
        pltpu.make_async_copy(up_hbm, up_w, weight_sem.at[1]),
        pltpu.make_async_copy(down_hbm, down_w, weight_sem.at[2]),
    ]
    for copy in small_copies:
        copy.start()
    for copy in mixer_copies[:6]:
        copy.start()
    barrier = pltpu.get_barrier_semaphore()
    for offset in range(1, peers):
        pl.semaphore_signal(
            barrier,
            inc=1,
            device_id=(peer_of(me, offset), core),
            device_id_type=pl.DeviceIdType.MESH,
        )
    pl.semaphore_signal(
        barrier, inc=1, device_id=(me, 1 - core), device_id_type=pl.DeviceIdType.MESH
    )
    for copy in small_copies[2:]:
        copy.wait()
    fill_transition(decay_ref, frequency_ref, step_ref, transition_ref)
    fill_routes(capacity, me, ids_ref, route_weight_ref, taken_ref, combine_ref)
    for copy in mixer_copies[6:]:
        copy.start()
    small_copies[0].wait()
    small_copies[1].wait()
    pl.semaphore_wait(barrier, peers)

    def remote(source, target, send_sem, recv_sem, ep_index, tp_index):
        return pltpu.make_async_remote_copy(
            src_ref=source,
            dst_ref=target,
            send_sem=send_sem,
            recv_sem=recv_sem,
            device_id=(ep_index, tp_index),
            device_id_type=pl.DeviceIdType.MESH,
        )

    own_start = pl.multiple_of(core * half_width, half_width)
    other_start = pl.multiple_of((1 - core) * half_width, half_width)
    own_columns = pl.ds(own_start, half_width)
    other_columns = pl.ds(other_start, half_width)
    narrow = jnp.bfloat16
    swap_rows = remote(
        residual_ref, residual_other, swap_send_sem.at[0], swap_recv_sem.at[0], me, 1 - core
    )
    swap_rows.start()
    start_rows = residual_ref[...].astype(jnp.float32)
    gained = (start_rows * mix_gain_ref[:, own_columns]).astype(narrow)
    squares = row_squares(start_rows)
    mixer_copies[0].wait()
    channels_sum = jnp.dot(gained, in_v[own_columns, :], preferred_element_type=jnp.float32)
    mixer_copies[1].wait()
    swap_rows.wait_recv()
    other_rows = residual_other[...].astype(jnp.float32)
    gained = (other_rows * mix_gain_ref[:, other_columns]).astype(narrow)
    squares = squares + row_squares(other_rows)
    channels_sum = channels_sum + jnp.dot(
        gained, in_v[other_columns, :], preferred_element_type=jnp.float32
    )
    channels = (channels_sum * lax.rsqrt(squares / (2 * half_width) + epsilon)).astype(narrow)
    for copy in weights:
        copy.start()

    mixer_width = channels.shape[1]
    entries = push_v.shape[2]
    wide = 128
    groups = wide // group_channels
    block = groups * entries
    shape = (wide, block)
    inside = (
        lax.broadcasted_iota(jnp.int32, shape, 0) // group_channels
        == lax.broadcasted_iota(jnp.int32, shape, 1) // entries
    )

    def block_diagonal(source, part, start):
        values = source[part, start : start + wide, :]
        return jnp.where(inside, jnp.concatenate([values] * groups, axis=1), 0.0).astype(narrow)

    for copy in mixer_copies[2:5]:
        copy.wait()
    for place in range(mixer_width // wide):
        start = place * wide
        states = slice(place * block, (place + 1) * block)
        inputs = channels[:, start : start + wide]
        raw_real = jnp.dot(
            inputs, block_diagonal(push_v, 0, start), preferred_element_type=jnp.float32
        )
        raw_imag = jnp.dot(
            inputs, block_diagonal(push_v, 1, start), preferred_element_type=jnp.float32
        )
        bar_real, bar_imag = transition_ref[0:1, states], transition_ref[1:2, states]
        coef_real, coef_imag = transition_ref[2:3, states], transition_ref[3:4, states]
        old_real, old_imag = state_v[0, :, states], state_v[1, :, states]
        new_real = (
            bar_real * old_real - bar_imag * old_imag + coef_real * raw_real - coef_imag * raw_imag
        )
        new_imag = (
            bar_real * old_imag + bar_imag * old_real + coef_real * raw_imag + coef_imag * raw_real
        )
        state_v[0, :, states] = new_real
        state_v[1, :, states] = new_imag
        transposed = (((1,), (1,)), ((), ()))
        mixed = (
            lax.dot_general(
                new_real.astype(narrow),
                block_diagonal(read_v, 0, start),
                transposed,
                preferred_element_type=jnp.float32,
            )
            - lax.dot_general(
                new_imag.astype(narrow),
                block_diagonal(read_v, 1, start),
                transposed,
                preferred_element_type=jnp.float32,
            )
            + passthrough_ref[:, start : start + wide] * inputs.astype(jnp.float32)
        )
        mixer_own[:, start : start + wide] = gelu_tanh(mixed).astype(narrow)
    swap_mixed = remote(
        mixer_own, mixer_other, swap_send_sem.at[1], swap_recv_sem.at[1], me, 1 - core
    )
    swap_mixed.start()
    own_channels = pl.ds(pl.multiple_of(core * mixer_width, mixer_width), mixer_width)
    other_channels = pl.ds(pl.multiple_of((1 - core) * mixer_width, mixer_width), mixer_width)
    mine = mixer_own[...].astype(jnp.float32)
    squares = row_squares(mine)
    mixer_copies[5].wait()
    projected = jnp.dot(
        (mine * out_gain_ref[:, own_channels]).astype(narrow),
        out_v[own_channels, :],
        preferred_element_type=jnp.float32,
    )
    swap_mixed.wait_recv()
    others = mixer_other[...].astype(jnp.float32)
    squares = squares + row_squares(others)
    projected = projected + jnp.dot(
        (others * out_gain_ref[:, other_channels]).astype(narrow),
        out_v[other_channels, :],
        preferred_element_type=jnp.float32,
    )
    after_rows = (
        start_rows + projected * lax.rsqrt(squares / (2 * mixer_width) + epsilon)
    ).astype(narrow)
    after_ref[...] = after_rows
    half = peers // 2
    middle = half + half // 2
    chunks = ((half, middle), (middle, peers), (0, half))
    pieces = ((half, middle), (middle, peers), (half // 2, half), (0, half // 2))
    outward = {}
    for first, last in pieces:
        slots = slice(first * capacity, last * capacity)
        buffer_ref[first:last] = (
            jnp.dot(taken_ref[slots, :], after_rows, preferred_element_type=jnp.float32)
            .reshape(last - first, capacity, half_width)
            .astype(narrow)
        )
        for offset in range(first, last):
            if not offset:
                continue
            outward[offset] = remote(
                buffer_ref.at[offset],
                rows_own.at[offset],
                go_send_sem.at[offset],
                go_recv_sem.at[offset],
                peer_of(me, offset),
                core,
            )
            outward[offset].start()
    rows_own[0] = buffer_ref[0]
    back = {}
    parts = []
    pairs = {}
    for chunk, (first, last) in enumerate(chunks):
        count = (last - first) * capacity
        for offset in range(first, last):
            if offset:
                outward[offset].wait_recv()
            source = rows_own.at[offset] if offset else buffer_ref.at[0]
            pairs[offset] = remote(
                source,
                rows_other.at[offset],
                pair_send_sem.at[offset],
                pair_recv_sem.at[offset],
                me,
                1 - core,
            )
            pairs[offset].start()
        own_rows = (
            rows_own[first:last]
            .astype(jnp.float32)
            .reshape(count, half_width)
        )
        for offset in range(first, last):
            pairs[offset].wait_recv()
        other_half = (
            rows_other[first:last]
            .astype(jnp.float32)
            .reshape(count, half_width)
        )
        row_scale = lax.rsqrt(
            (row_squares(own_rows) + row_squares(other_half)) / (2 * half_width) + epsilon
        )
        flat[0:count, own_columns] = (own_rows * row_scale * ffn_gain_ref[:, own_columns]).astype(narrow)
        flat[0:count, other_columns] = (other_half * row_scale * ffn_gain_ref[:, other_columns]).astype(narrow)
        if chunk == 0:
            weights[0].wait()
            weights[1].wait()

        def hidden_tile(step, carry, count=count):
            columns = pl.ds(pl.multiple_of(step * tile, tile), tile)

            def both(weight):
                return jnp.dot(
                    flat[0:count], weight[:, columns], preferred_element_type=jnp.float32
                )

            gated = jnp.minimum(both(gate_w), clamp_limit)
            raised = jnp.clip(both(up_w), -clamp_limit, clamp_limit) + 1.0
            activation[0:count, columns] = (
                raised * gated * (1.0 / (1.0 + jnp.exp(-swish_alpha * gated)))
            ).astype(jnp.bfloat16)
            return carry

        lax.fori_loop(0, hidden // tile, hidden_tile, 0)
        if chunk == 0:
            weights[2].wait()

        def down_tiles(start, target):
            def down_tile(step, carry, count=count):
                columns = pl.ds(pl.multiple_of(step * tile, tile), tile)
                source = pl.ds(pl.multiple_of(start + step * tile, tile), tile)
                target[0:count, columns] = jnp.dot(
                    activation[0:count], down_w[:, source], preferred_element_type=jnp.float32
                ).astype(jnp.bfloat16)
                return carry

            lax.fori_loop(0, half_width // tile, down_tile, 0)

        down_tiles(other_start, part_send.at[chunk])
        parts.append(
            remote(
                part_send.at[chunk, pl.ds(0, count)],
                part_recv.at[chunk, pl.ds(0, count)],
                part_send_sem.at[chunk],
                part_recv_sem.at[chunk],
                me,
                1 - core,
            )
        )
        parts[chunk].start()
        down_tiles(own_start, part_own)
        parts[chunk].wait_recv()
        back_send[first:last] = (
            (part_own[0:count].astype(jnp.float32) + part_recv[chunk, 0:count].astype(jnp.float32))
            .reshape(last - first, capacity, half_width)
            .astype(jnp.bfloat16)
        )
        for offset in range(first, last):
            if offset == 0:
                back_recv[0] = back_send[0]
                continue
            peer = peer_of(me, offset)
            back[offset] = remote(
                back_send.at[offset],
                back_recv.at[offset],
                back_send_sem.at[offset],
                back_recv_sem.at[offset],
                peer,
                core,
            )
            back[offset].start()
    over_slots = (((0,), (0,)), ((), ()))
    total = after_ref[...].astype(jnp.float32)
    for first, last in chunks:
        for offset in range(max(1, first), last):
            back[offset].wait_recv()
        returned = (
            back_recv[first:last]
            .astype(jnp.float32)
            .reshape((last - first) * capacity, half_width)
            .astype(jnp.bfloat16)
        )
        weight = combine_ref[first * capacity : last * capacity, :]
        high = weight.astype(jnp.bfloat16)
        low = (weight - high.astype(jnp.float32)).astype(jnp.bfloat16)
        total = total + (
            lax.dot_general(high, returned, over_slots, preferred_element_type=jnp.float32)
            + lax.dot_general(low, returned, over_slots, preferred_element_type=jnp.float32)
        )
    out_ref[...] = total.astype(jnp.bfloat16)
    for offset in range(1, peers):
        outward[offset].wait_send()
        back[offset].wait_send()
    for offset in range(peers):
        pairs[offset].wait_send()
    for copy in parts:
        copy.wait_send()
    swap_rows.wait_send()
    swap_mixed.wait_send()


def layer_call(group_channels, peers, capacity, residual, *operands):
    state, in_proj, push_map, read_map, out_proj, w_gate, w_up, w_down = operands[9:]
    half_width = residual.shape[1]
    rows = peers // 2 * capacity
    narrow = jnp.bfloat16
    blocks = pltpu.VMEM((peers, capacity, half_width), narrow)
    flat = pltpu.VMEM((rows, half_width), narrow)
    mixer = pltpu.VMEM((residual.shape[0], in_proj.shape[1]), narrow)
    dma = pltpu.SemaphoreType.DMA
    vmem = pl.BlockSpec(memory_space=pltpu.VMEM)
    anywhere = pl.BlockSpec(memory_space=pl.ANY)
    return pl.pallas_call(
        functools.partial(layer_kernel, peers, capacity, group_channels),
        out_shape=(
            pltpu.VMEM(residual.shape, narrow),
            pltpu.VMEM(state.shape, jnp.float32),
        ),
        in_specs=[anywhere] * 18,
        out_specs=(vmem, vmem),
        scratch_shapes=[
            pltpu.VMEM(residual.shape, narrow),
            *[pltpu.VMEM(one.shape, one.dtype) for one in operands[:9]],
            pltpu.VMEM(in_proj.shape, narrow),
            pltpu.VMEM(push_map.shape, jnp.float32),
            pltpu.VMEM(read_map.shape, jnp.float32),
            pltpu.VMEM(out_proj.shape, narrow),
            pltpu.VMEM(residual.shape, narrow),
            mixer,
            mixer,
            pltpu.VMEM(residual.shape, narrow),
            pltpu.VMEM((4, state.shape[2]), jnp.float32),
            pltpu.VMEM((peers * capacity, residual.shape[0]), narrow),
            pltpu.VMEM((peers * capacity, residual.shape[0]), jnp.float32),
            blocks,
            pltpu.VMEM(w_gate.shape, narrow),
            pltpu.VMEM(w_up.shape, narrow),
            pltpu.VMEM(w_down.shape, narrow),
            blocks,
            blocks,
            pltpu.VMEM((rows, 2 * half_width), narrow),
            pltpu.VMEM((rows, w_gate.shape[1]), narrow),
            pltpu.VMEM((3, rows, half_width), narrow),
            pltpu.VMEM((3, rows, half_width), narrow),
            flat,
            blocks,
            blocks,
            dma((10,)),
            dma((3,)),
            dma((6,)),
            dma((2,)),
            dma((2,)),
            dma((peers,)),
            dma((peers,)),
            dma((peers,)),
            dma((peers,)),
            dma((3,)),
            dma((3,)),
            dma((peers,)),
            dma((peers,)),
        ],
        compiler_params=pltpu.CompilerParams(
            collective_id=0, has_side_effects=True, vmem_limit_bytes=56 * 1024 * 1024
        ),
    )(residual, *operands)


def local(
    residual,
    route_ids,
    route_weights,
    carried_state,
    mix_gain,
    in_proj,
    decay_rate,
    frequency,
    step_size,
    input_map,
    output_matrix,
    passthrough_scale,
    out_gain,
    out_proj,
    ffn_gain,
    w_gate,
    w_up,
    w_down,
):
    row_count, half_width = residual.shape
    top_count = route_ids.shape[1]
    local_experts = w_gate.shape[0]
    peer_count = lax.axis_size("ep")
    expert_count = local_experts * peer_count
    capacity = max(2, 3 * row_count * top_count // (2 * expert_count))
    capacity = -(-capacity // 8) * 8
    push_map = jnp.swapaxes(input_map, 2, 3).reshape(2, -1, input_map.shape[2])
    read_map = output_matrix.reshape(2, -1, output_matrix.shape[3])
    updated, new_state = layer_call(
        input_map.shape[3],
        peer_count,
        capacity,
        residual,
        route_ids.T,
        route_weights.T,
        mix_gain[None, :],
        decay_rate,
        frequency,
        step_size[None, :],
        passthrough_scale[None, :],
        out_gain[None, :],
        ffn_gain[None, :],
        carried_state,
        in_proj,
        push_map,
        read_map,
        out_proj,
        w_gate[0],
        w_up[0],
        w_down[0],
    )
    return (updated, new_state)


def solution(mesh):
    placed = (
        P("ep", "tp"),
        P("ep", None),
        P("ep", None),
        P(None, "ep", "tp"),
        P(),
        P(None, "tp"),
        P("tp", None),
        P("tp", None),
        P("tp"),
        P(None, "tp", None, None),
        P(None, "tp", None, None),
        P("tp"),
        P(),
        P(None, "tp"),
        P(),
        P("ep", None, "tp"),
        P("ep", None, "tp"),
        P("ep", "tp", None),
    )
    return jax.shard_map(
        local,
        mesh=mesh,
        in_specs=placed,
        out_specs=(P("ep", "tp"), P(None, "ep", "tp")),
        check_vma=False,
    )
```

```python
import functools
import jax
import jax.numpy as jnp
from jax import lax
from jax.experimental import pallas as pl
from jax.experimental.pallas import tpu as pltpu
from jax.sharding import PartitionSpec as P

epsilon = 1e-06
clamp_limit = 7.0
swish_alpha = 1.702


line_order = (2, 3, 1, 0)


def discretize(decay_rate, frequency, step_size):
    rate_real = -decay_rate
    time_step = step_size
    magnitude = jnp.exp(rate_real * time_step)
    phase_angle = frequency * time_step
    bar_real = magnitude * jnp.cos(phase_angle)
    bar_imag = magnitude * jnp.sin(phase_angle)
    denominator = rate_real * rate_real + frequency * frequency
    shifted = bar_real - 1.0
    coef_real = (shifted * rate_real + bar_imag * frequency) / denominator
    coef_imag = (bar_imag * rate_real - shifted * frequency) / denominator
    return (bar_real, bar_imag, coef_real, coef_imag)


def peer_of(index, offset):
    out = index
    bit = 1
    while bit <= offset:
        if offset & bit:
            out = out + bit * (1 - 2 * ((index // bit) % 2))
        bit *= 2
    return out


def gelu_tanh(value):
    inner = 0.7978845608028654 * (value + 0.044715 * value * value * value)
    return 0.5 * value * (1.0 + jnp.tanh(inner))


def row_squares(value):
    return jnp.sum(value * value, axis=1, keepdims=True)


def fill_transition(decay_ref, frequency_ref, step_ref, transition_ref):
    groups, entries = decay_ref.shape
    diagonal = lax.broadcasted_iota(jnp.int32, (groups, groups), 0) == lax.broadcasted_iota(
        jnp.int32, (groups, groups), 1
    )
    steps = jnp.sum(jnp.where(diagonal, step_ref[...], 0.0), axis=1, keepdims=True)
    shape = (groups, groups * entries)
    inside = (
        lax.broadcasted_iota(jnp.int32, shape, 0)
        == lax.broadcasted_iota(jnp.int32, shape, 1) // entries
    )
    for place, term in enumerate(discretize(decay_ref[...], frequency_ref[...], steps)):
        spread = jnp.concatenate([term] * groups, axis=1)
        transition_ref[place : place + 1, :] = jnp.sum(
            jnp.where(inside, spread, 0.0), axis=0, keepdims=True
        )


def fill_routes(capacity, me, ids_ref, route_weight_ref, taken_ref, combine_ref):
    top_count, rows = ids_ref.shape
    experts = taken_ref.shape[0] // capacity
    place = lax.broadcasted_iota(jnp.int32, (experts, rows), 0)
    quarter = experts // 4
    block = jnp.zeros((experts, rows), jnp.int32)
    for turn, line in enumerate(line_order):
        block = jnp.where(place // quarter == turn, line, block)
    expert_iota = jnp.bitwise_xor(block * quarter + place % quarter, me)
    chosen = jnp.zeros((experts, rows), jnp.float32)
    weight = jnp.zeros((experts, rows), jnp.float32)
    for choice in range(top_count):
        named = ids_ref[choice : choice + 1, :] == expert_iota
        chosen = jnp.where(named, 1.0, chosen)
        weight = jnp.where(named, route_weight_ref[choice : choice + 1, :], weight)
    earlier = jnp.where(
        lax.broadcasted_iota(jnp.int32, (rows, rows), 0)
        < lax.broadcasted_iota(jnp.int32, (rows, rows), 1),
        1.0,
        0.0,
    ).astype(jnp.bfloat16)
    before = jnp.dot(
        chosen.astype(jnp.bfloat16), earlier, preferred_element_type=jnp.float32
    )
    slot = jnp.where(chosen > 0.0, before, -1.0)
    slot_iota = lax.broadcasted_iota(jnp.int32, (capacity, rows), 0).astype(jnp.float32)
    for expert in range(experts):
        lines = slice(expert * capacity, (expert + 1) * capacity)
        taken = slot[expert : expert + 1, :] == slot_iota
        taken_ref[lines, :] = jnp.where(taken, 1.0, 0.0).astype(jnp.bfloat16)
        combine_ref[lines, :] = jnp.where(taken, weight[expert : expert + 1, :], 0.0)


def layer_kernel(
    peers,
    capacity,
    group_channels,
    residual_hbm,
    ids_hbm,
    route_weight_hbm,
    mix_gain_hbm,
    decay_hbm,
    frequency_hbm,
    step_hbm,
    passthrough_hbm,
    out_gain_hbm,
    ffn_gain_hbm,
    state_hbm,
    in_hbm,
    push_hbm,
    read_hbm,
    out_hbm,
    gate_hbm,
    up_hbm,
    down_hbm,
    out_ref,
    state_v,
    residual_ref,
    ids_ref,
    route_weight_ref,
    mix_gain_ref,
    decay_ref,
    frequency_ref,
    step_ref,
    passthrough_ref,
    out_gain_ref,
    ffn_gain_ref,
    in_v,
    push_v,
    read_v,
    out_v,
    residual_other,
    mixer_own,
    mixer_other,
    after_ref,
    transition_ref,
    taken_ref,
    combine_ref,
    buffer_ref,
    gate_w,
    up_w,
    down_w,
    rows_own,
    rows_other,
    flat,
    activation,
    part_send,
    part_recv,
    part_own,
    back_send,
    back_recv,
    small_sem,
    weight_sem,
    mixer_sem,
    swap_send_sem,
    swap_recv_sem,
    go_send_sem,
    go_recv_sem,
    pair_send_sem,
    pair_recv_sem,
    part_send_sem,
    part_recv_sem,
    back_send_sem,
    back_recv_sem,
):
    me = lax.axis_index("ep")
    core = lax.axis_index("tp")
    half_width = residual_hbm.shape[1]
    hidden = gate_w.shape[1]
    tile = 1024
    half_rows = residual_hbm.shape[1]
    first_half = pl.ds(pl.multiple_of(core * half_rows, half_rows), half_rows)
    second_half = pl.ds(pl.multiple_of((1 - core) * half_rows, half_rows), half_rows)
    small_copies = [
        pltpu.make_async_copy(source, target, small_sem.at[place])
        for place, (source, target) in enumerate(
            (
                (residual_hbm, residual_ref),
                (mix_gain_hbm, mix_gain_ref),
                (ids_hbm, ids_ref),
                (route_weight_hbm, route_weight_ref),
                (decay_hbm, decay_ref),
                (frequency_hbm, frequency_ref),
                (step_hbm, step_ref),
                (passthrough_hbm, passthrough_ref),
                (out_gain_hbm, out_gain_ref),
                (ffn_gain_hbm, ffn_gain_ref),
            )
        )
    ]
    mixer_copies = [
        pltpu.make_async_copy(source, target, mixer_sem.at[place])
        for place, (source, target) in enumerate(
            (
                (in_hbm.at[first_half], in_v.at[first_half]),
                (in_hbm.at[second_half], in_v.at[second_half]),
                (push_hbm, push_v),
                (state_hbm, state_v),
                (read_hbm, read_v),
                (out_hbm, out_v),
            )
        )
    ]
    weights = [
        pltpu.make_async_copy(gate_hbm, gate_w, weight_sem.at[0]),
        pltpu.make_async_copy(up_hbm, up_w, weight_sem.at[1]),
        pltpu.make_async_copy(down_hbm, down_w, weight_sem.at[2]),
    ]
    for copy in small_copies:
        copy.start()
    for copy in mixer_copies[:6]:
        copy.start()
    barrier = pltpu.get_barrier_semaphore()
    for offset in range(1, peers):
        pl.semaphore_signal(
            barrier,
            inc=1,
            device_id=(peer_of(me, offset), core),
            device_id_type=pl.DeviceIdType.MESH,
        )
    pl.semaphore_signal(
        barrier, inc=1, device_id=(me, 1 - core), device_id_type=pl.DeviceIdType.MESH
    )
    for copy in small_copies[2:]:
        copy.wait()
    fill_transition(decay_ref, frequency_ref, step_ref, transition_ref)
    fill_routes(capacity, me, ids_ref, route_weight_ref, taken_ref, combine_ref)
    for copy in mixer_copies[6:]:
        copy.start()
    small_copies[0].wait()
    small_copies[1].wait()
    pl.semaphore_wait(barrier, peers)

    def remote(source, target, send_sem, recv_sem, ep_index, tp_index):
        return pltpu.make_async_remote_copy(
            src_ref=source,
            dst_ref=target,
            send_sem=send_sem,
            recv_sem=recv_sem,
            device_id=(ep_index, tp_index),
            device_id_type=pl.DeviceIdType.MESH,
        )

    own_start = pl.multiple_of(core * half_width, half_width)
    other_start = pl.multiple_of((1 - core) * half_width, half_width)
    own_columns = pl.ds(own_start, half_width)
    other_columns = pl.ds(other_start, half_width)
    narrow = jnp.bfloat16
    swap_rows = remote(
        residual_ref, residual_other, swap_send_sem.at[0], swap_recv_sem.at[0], me, 1 - core
    )
    swap_rows.start()
    start_rows = residual_ref[...].astype(jnp.float32)
    gained = (start_rows * mix_gain_ref[:, own_columns]).astype(narrow)
    squares = row_squares(start_rows)
    mixer_copies[0].wait()
    channels_sum = jnp.dot(gained, in_v[own_columns, :], preferred_element_type=jnp.float32)
    mixer_copies[1].wait()
    swap_rows.wait_recv()
    other_rows = residual_other[...].astype(jnp.float32)
    gained = (other_rows * mix_gain_ref[:, other_columns]).astype(narrow)
    squares = squares + row_squares(other_rows)
    channels_sum = channels_sum + jnp.dot(
        gained, in_v[other_columns, :], preferred_element_type=jnp.float32
    )
    channels = (channels_sum * lax.rsqrt(squares / (2 * half_width) + epsilon)).astype(narrow)
    for copy in weights:
        copy.start()

    mixer_width = channels.shape[1]
    entries = push_v.shape[2]
    wide = 128
    groups = wide // group_channels
    block = groups * entries
    shape = (wide, block)
    inside = (
        lax.broadcasted_iota(jnp.int32, shape, 0) // group_channels
        == lax.broadcasted_iota(jnp.int32, shape, 1) // entries
    )

    def block_diagonal(source, part, start):
        values = source[part, start : start + wide, :]
        return jnp.where(inside, jnp.concatenate([values] * groups, axis=1), 0.0).astype(narrow)

    for copy in mixer_copies[2:5]:
        copy.wait()
    for place in range(mixer_width // wide):
        start = place * wide
        states = slice(place * block, (place + 1) * block)
        inputs = channels[:, start : start + wide]
        raw_real = jnp.dot(
            inputs, block_diagonal(push_v, 0, start), preferred_element_type=jnp.float32
        )
        raw_imag = jnp.dot(
            inputs, block_diagonal(push_v, 1, start), preferred_element_type=jnp.float32
        )
        bar_real, bar_imag = transition_ref[0:1, states], transition_ref[1:2, states]
        coef_real, coef_imag = transition_ref[2:3, states], transition_ref[3:4, states]
        old_real, old_imag = state_v[0, :, states], state_v[1, :, states]
        new_real = (
            bar_real * old_real - bar_imag * old_imag + coef_real * raw_real - coef_imag * raw_imag
        )
        new_imag = (
            bar_real * old_imag + bar_imag * old_real + coef_real * raw_imag + coef_imag * raw_real
        )
        state_v[0, :, states] = new_real
        state_v[1, :, states] = new_imag
        transposed = (((1,), (1,)), ((), ()))
        mixed = (
            lax.dot_general(
                new_real.astype(narrow),
                block_diagonal(read_v, 0, start),
                transposed,
                preferred_element_type=jnp.float32,
            )
            - lax.dot_general(
                new_imag.astype(narrow),
                block_diagonal(read_v, 1, start),
                transposed,
                preferred_element_type=jnp.float32,
            )
            + passthrough_ref[:, start : start + wide] * inputs.astype(jnp.float32)
        )
        mixer_own[:, start : start + wide] = gelu_tanh(mixed).astype(narrow)
    swap_mixed = remote(
        mixer_own, mixer_other, swap_send_sem.at[1], swap_recv_sem.at[1], me, 1 - core
    )
    swap_mixed.start()
    own_channels = pl.ds(pl.multiple_of(core * mixer_width, mixer_width), mixer_width)
    other_channels = pl.ds(pl.multiple_of((1 - core) * mixer_width, mixer_width), mixer_width)
    mine = mixer_own[...].astype(jnp.float32)
    squares = row_squares(mine)
    mixer_copies[5].wait()
    projected = jnp.dot(
        (mine * out_gain_ref[:, own_channels]).astype(narrow),
        out_v[own_channels, :],
        preferred_element_type=jnp.float32,
    )
    swap_mixed.wait_recv()
    others = mixer_other[...].astype(jnp.float32)
    squares = squares + row_squares(others)
    projected = projected + jnp.dot(
        (others * out_gain_ref[:, other_channels]).astype(narrow),
        out_v[other_channels, :],
        preferred_element_type=jnp.float32,
    )
    after_rows = (
        start_rows + projected * lax.rsqrt(squares / (2 * mixer_width) + epsilon)
    ).astype(narrow)
    after_ref[...] = after_rows
    quarter = peers // 4
    offsets = [line * quarter + spot for line in line_order for spot in range(quarter)]
    own_place = offsets.index(0)
    chunks = tuple((first * quarter, last * quarter) for first, last in ((0, 1), (1, 3), (3, 4)))
    outward = {}
    for block in (0, 1, 2, 3):
        first, last = block * quarter, (block + 1) * quarter
        slots = slice(first * capacity, last * capacity)
        buffer_ref[first:last] = (
            jnp.dot(taken_ref[slots, :], after_rows, preferred_element_type=jnp.float32)
            .reshape(quarter, capacity, half_width)
            .astype(narrow)
        )
        for place in range(first, last):
            if place == own_place:
                continue
            outward[place] = remote(
                buffer_ref.at[place],
                rows_own.at[place],
                go_send_sem.at[place],
                go_recv_sem.at[place],
                peer_of(me, offsets[place]),
                core,
            )
            outward[place].start()
    rows_own[own_place] = buffer_ref[own_place]
    back = {}
    parts = []
    pairs = {}
    for chunk, (first, last) in enumerate(chunks):
        count = (last - first) * capacity
        for place in range(first, last):
            if place != own_place:
                outward[place].wait_recv()
            source = rows_own.at[place] if place != own_place else buffer_ref.at[place]
            pairs[place] = remote(
                source,
                rows_other.at[place],
                pair_send_sem.at[place],
                pair_recv_sem.at[place],
                me,
                1 - core,
            )
            pairs[place].start()
        own_rows = (
            rows_own[first:last]
            .astype(jnp.float32)
            .reshape(count, half_width)
        )
        for offset in range(first, last):
            pairs[offset].wait_recv()
        other_half = (
            rows_other[first:last]
            .astype(jnp.float32)
            .reshape(count, half_width)
        )
        row_scale = lax.rsqrt(
            (row_squares(own_rows) + row_squares(other_half)) / (2 * half_width) + epsilon
        )
        flat[0:count, own_columns] = (own_rows * row_scale * ffn_gain_ref[:, own_columns]).astype(narrow)
        flat[0:count, other_columns] = (other_half * row_scale * ffn_gain_ref[:, other_columns]).astype(narrow)
        if chunk == 0:
            weights[0].wait()
            weights[1].wait()

        def hidden_tile(step, carry, count=count):
            columns = pl.ds(pl.multiple_of(step * tile, tile), tile)

            def both(weight):
                return jnp.dot(
                    flat[0:count], weight[:, columns], preferred_element_type=jnp.float32
                )

            gated = jnp.minimum(both(gate_w), clamp_limit)
            raised = jnp.clip(both(up_w), -clamp_limit, clamp_limit) + 1.0
            activation[0:count, columns] = (
                raised * gated * (1.0 / (1.0 + jnp.exp(-swish_alpha * gated)))
            ).astype(jnp.bfloat16)
            return carry

        lax.fori_loop(0, hidden // tile, hidden_tile, 0)
        if chunk == 0:
            weights[2].wait()

        def down_tiles(start, target):
            def down_tile(step, carry, count=count):
                columns = pl.ds(pl.multiple_of(step * tile, tile), tile)
                source = pl.ds(pl.multiple_of(start + step * tile, tile), tile)
                target[0:count, columns] = jnp.dot(
                    activation[0:count], down_w[:, source], preferred_element_type=jnp.float32
                ).astype(jnp.bfloat16)
                return carry

            lax.fori_loop(0, half_width // tile, down_tile, 0)

        down_tiles(other_start, part_send.at[chunk])
        parts.append(
            remote(
                part_send.at[chunk, pl.ds(0, count)],
                part_recv.at[chunk, pl.ds(0, count)],
                part_send_sem.at[chunk],
                part_recv_sem.at[chunk],
                me,
                1 - core,
            )
        )
        parts[chunk].start()
        down_tiles(own_start, part_own)
        parts[chunk].wait_recv()
        back_send[first:last] = (
            (part_own[0:count].astype(jnp.float32) + part_recv[chunk, 0:count].astype(jnp.float32))
            .reshape(last - first, capacity, half_width)
            .astype(jnp.bfloat16)
        )
        for place in range(first, last):
            if place == own_place:
                back_recv[place] = back_send[place]
                continue
            back[place] = remote(
                back_send.at[place],
                back_recv.at[place],
                back_send_sem.at[place],
                back_recv_sem.at[place],
                peer_of(me, offsets[place]),
                core,
            )
            back[place].start()
    over_slots = (((0,), (0,)), ((), ()))
    total = after_ref[...].astype(jnp.float32)
    for first, last in chunks:
        for place in range(first, last):
            if place != own_place:
                back[place].wait_recv()
        returned = (
            back_recv[first:last]
            .astype(jnp.float32)
            .reshape((last - first) * capacity, half_width)
            .astype(jnp.bfloat16)
        )
        weight = combine_ref[first * capacity : last * capacity, :]
        high = weight.astype(jnp.bfloat16)
        low = (weight - high.astype(jnp.float32)).astype(jnp.bfloat16)
        total = total + (
            lax.dot_general(high, returned, over_slots, preferred_element_type=jnp.float32)
            + lax.dot_general(low, returned, over_slots, preferred_element_type=jnp.float32)
        )
    out_ref[...] = total.astype(jnp.bfloat16)
    for place in outward:
        outward[place].wait_send()
        back[place].wait_send()
    for offset in range(peers):
        pairs[offset].wait_send()
    for copy in parts:
        copy.wait_send()
    swap_rows.wait_send()
    swap_mixed.wait_send()


def layer_call(group_channels, peers, capacity, residual, *operands):
    state, in_proj, push_map, read_map, out_proj, w_gate, w_up, w_down = operands[9:]
    half_width = residual.shape[1]
    rows = peers // 2 * capacity
    narrow = jnp.bfloat16
    blocks = pltpu.VMEM((peers, capacity, half_width), narrow)
    flat = pltpu.VMEM((rows, half_width), narrow)
    mixer = pltpu.VMEM((residual.shape[0], in_proj.shape[1]), narrow)
    dma = pltpu.SemaphoreType.DMA
    vmem = pl.BlockSpec(memory_space=pltpu.VMEM)
    anywhere = pl.BlockSpec(memory_space=pl.ANY)
    return pl.pallas_call(
        functools.partial(layer_kernel, peers, capacity, group_channels),
        out_shape=(
            pltpu.VMEM(residual.shape, narrow),
            pltpu.VMEM(state.shape, jnp.float32),
        ),
        in_specs=[anywhere] * 18,
        out_specs=(vmem, vmem),
        scratch_shapes=[
            pltpu.VMEM(residual.shape, narrow),
            *[pltpu.VMEM(one.shape, one.dtype) for one in operands[:9]],
            pltpu.VMEM(in_proj.shape, narrow),
            pltpu.VMEM(push_map.shape, jnp.float32),
            pltpu.VMEM(read_map.shape, jnp.float32),
            pltpu.VMEM(out_proj.shape, narrow),
            pltpu.VMEM(residual.shape, narrow),
            mixer,
            mixer,
            pltpu.VMEM(residual.shape, narrow),
            pltpu.VMEM((4, state.shape[2]), jnp.float32),
            pltpu.VMEM((peers * capacity, residual.shape[0]), narrow),
            pltpu.VMEM((peers * capacity, residual.shape[0]), jnp.float32),
            blocks,
            pltpu.VMEM(w_gate.shape, narrow),
            pltpu.VMEM(w_up.shape, narrow),
            pltpu.VMEM(w_down.shape, narrow),
            blocks,
            blocks,
            pltpu.VMEM((rows, 2 * half_width), narrow),
            pltpu.VMEM((rows, w_gate.shape[1]), narrow),
            pltpu.VMEM((3, rows, half_width), narrow),
            pltpu.VMEM((3, rows, half_width), narrow),
            flat,
            blocks,
            blocks,
            dma((10,)),
            dma((3,)),
            dma((6,)),
            dma((2,)),
            dma((2,)),
            dma((peers,)),
            dma((peers,)),
            dma((peers,)),
            dma((peers,)),
            dma((3,)),
            dma((3,)),
            dma((peers,)),
            dma((peers,)),
        ],
        compiler_params=pltpu.CompilerParams(
            collective_id=0, has_side_effects=True, vmem_limit_bytes=56 * 1024 * 1024
        ),
    )(residual, *operands)


def local(
    residual,
    route_ids,
    route_weights,
    carried_state,
    mix_gain,
    in_proj,
    decay_rate,
    frequency,
    step_size,
    input_map,
    output_matrix,
    passthrough_scale,
    out_gain,
    out_proj,
    ffn_gain,
    w_gate,
    w_up,
    w_down,
):
    row_count, half_width = residual.shape
    top_count = route_ids.shape[1]
    local_experts = w_gate.shape[0]
    peer_count = lax.axis_size("ep")
    expert_count = local_experts * peer_count
    capacity = max(2, 3 * row_count * top_count // (2 * expert_count))
    capacity = -(-capacity // 8) * 8
    push_map = jnp.swapaxes(input_map, 2, 3).reshape(2, -1, input_map.shape[2])
    read_map = output_matrix.reshape(2, -1, output_matrix.shape[3])
    updated, new_state = layer_call(
        input_map.shape[3],
        peer_count,
        capacity,
        residual,
        route_ids.T,
        route_weights.T,
        mix_gain[None, :],
        decay_rate,
        frequency,
        step_size[None, :],
        passthrough_scale[None, :],
        out_gain[None, :],
        ffn_gain[None, :],
        carried_state,
        in_proj,
        push_map,
        read_map,
        out_proj,
        w_gate[0],
        w_up[0],
        w_down[0],
    )
    return (updated, new_state)


def solution(mesh):
    placed = (
        P("ep", "tp"),
        P("ep", None),
        P("ep", None),
        P(None, "ep", "tp"),
        P(),
        P(None, "tp"),
        P("tp", None),
        P("tp", None),
        P("tp"),
        P(None, "tp", None, None),
        P(None, "tp", None, None),
        P("tp"),
        P(),
        P(None, "tp"),
        P(),
        P("ep", None, "tp"),
        P("ep", None, "tp"),
        P("ep", "tp", None),
    )
    return jax.shard_map(
        local,
        mesh=mesh,
        in_specs=placed,
        out_specs=(P("ep", "tp"), P(None, "ep", "tp")),
        check_vma=False,
    )
```
